32 devices in a mesh: dp: 4 (over y, x), kv: 4 (over z), tp: 2 (over core).
Axes of the slice: x: 2, y: 2, z: 4, core: 2. Of those that a mesh axis runs over, the one named last changes fastest.
Arguments:
- tokens: bfloat16 [8192, 1024], P(('dp', 'kv')), parts along dimension 0, may hold values from -6 to 6
- chosen: int32 [128, 2, 16], P(('dp', 'kv'), 'tp'), parts along dimension 0, may hold values from 0 to 31, as said below
- w_query: bfloat16 [1024, 512], P(None, 'tp'), may hold values from -0.1875 to 0.1875
- w_key_summary: bfloat16 [1024, 128], replicated, may hold values from -0.1875 to 0.1875
- w_value_summary: bfloat16 [1024, 128], replicated, may hold values from -0.1875 to 0.1875
- w_key_chosen: bfloat16 [1024, 128], replicated, may hold values from -0.1875 to 0.1875
- w_value_chosen: bfloat16 [1024, 128], replicated, may hold values from -0.1875 to 0.1875
- squeeze_key_in: bfloat16 [2048, 64], replicated, may hold values from -0.125 to 0.125
- squeeze_key_out: bfloat16 [64, 64], replicated, may hold values from -0.75 to 0.75
- squeeze_value_in: bfloat16 [2048, 64], replicated, may hold values from -0.125 to 0.125
- squeeze_value_out: bfloat16 [64, 64], replicated, may hold values from -0.75 to 0.75
- w_gates: bfloat16 [1024, 16], replicated, may hold values from -0.1875 to 0.1875
- w_out: bfloat16 [512, 1024], replicated, may hold values from -0.25 to 0.25
- out_gain: float32 [1024], replicated, may hold values from 0.1 to 1.9
Outputs:
- attended: bfloat16 [8192, 1024], P(('dp', 'kv'), 'tp'), parts along dimension 0
The draws below stay inside these ranges and needn't reach their ends.
There are 4 independent parts, one for each index of `dp`. The reference program is written for one: setup_inputs(seed, part) draws one part's arguments, and reference() takes and returns one part's arrays. A program takes and returns all parts, laid end to end along the dimension named above; an argument that names none is the same for every part. Nothing has to cross between parts.
Inputs may be any that keep to these rules, and one draw needn't show every extreme that they name: The 16 blocks chosen by each query block and group are different and include the query block's own block; listed blocks after the query block have all their keys masked. Over the 8 query blocks of one aligned span of 512 positions and one group, at most 4 different chosen blocks lie in any other aligned span, and in every draw some span and group reaches 4.
All inputs are finite; a program needn't handle non-finite values.
Results may differ from the reference program's by a relative error of at most 0.005.
Values may be sent and summed in bfloat16 or wider, within the bound.
A program may use at most 128 MiB of HBM per device.

```python
import jax
import jax.numpy as jnp
from jax import lax

D = 1024
HEADS = 8
GROUPS = 2
HEAD = 64
CMP_STRIDE = 16
CMP_LEN = 32
SEL = 64
TOPK = 16
CAP = 4
SEQ = 2048
NB_DEV = 8
SEGMENT_TALLY = 32


def draw_chosen(key, part):
    owners_count = SEGMENT_TALLY // NB_DEV
    block_ids = jnp.arange(SEGMENT_TALLY).astype(jnp.int32)
    segment_holder = block_ids // NB_DEV
    block_local = block_ids % NB_DEV
    half_away = owners_count // 2
    results = []
    for group_index in range(GROUPS):
        group_key = jax.random.fold_in(key, 11 + group_index)
        menu_key, selection_seed = jax.random.split(group_key)
        menu_scores = jax.random.randint(menu_key, (owners_count, owners_count, NB_DEV), 0, 1 << 20) * NB_DEV + jnp.arange(NB_DEV)
        menu_rank = jnp.argsort(jnp.argsort(menu_scores, axis=-1), axis=-1)
        in_menu = menu_rank < CAP
        menu_hit = in_menu[segment_holder[:, None], segment_holder[None, :], block_local[None, :]]
        same_owner = segment_holder[:, None] == segment_holder[None, :]
        earlier = block_ids[None, :] <= block_ids[:, None]
        own_block = block_ids[None, :] == block_ids[:, None]
        last_local = (block_local == NB_DEV - 1)[:, None]
        neighbour = segment_holder[None, :] == segment_holder[:, None] - 1
        opposite = (segment_holder[None, :] == segment_holder[:, None] - half_away) & (half_away > 0)
        forced = last_local & menu_hit & (neighbour | opposite)
        allowed = same_owner | menu_hit
        causal = allowed & earlier
        extra_reward = jnp.where(segment_holder == 0, 600, 0)[None, :]
        jitter_amount = jax.random.randint(selection_seed, (SEGMENT_TALLY, SEGMENT_TALLY), 0, 1024) + extra_reward
        level = jnp.where(own_block, 4, jnp.where(forced, 3, jnp.where(causal, 2, jnp.where(allowed, 1, 0))))
        scores = level * (2048 * SEGMENT_TALLY) + jitter_amount * SEGMENT_TALLY + block_ids[None, :]
        unused, top_ids = lax.top_k(scores, TOPK)
        results.append(top_ids.astype(jnp.int32))
    return jnp.stack(results, axis=1)


def levels(key, extent, shards, low, largest):
    gain = 1.0
    for dim, blocks in shards:
        heights = jax.random.uniform(jax.random.fold_in(jax.random.fold_in(key, 6), dim), (blocks,), jnp.float32, low / len(shards), largest / len(shards))
        gain = gain * jnp.repeat(jnp.exp(heights), extent[dim] // blocks).reshape((-1,) + (1,) * (len(extent) - 1 - dim))
    return gain


def gaussian(own_key, dims, scale, bound, cuts=(), kind=jnp.bfloat16):
    entries = jax.random.normal(own_key, dims, jnp.float32) * scale
    if len(cuts) > 0:
        entries = levels(own_key, dims, cuts, -0.22, 0.18) * entries
    return jnp.clip(entries, min=-bound, max=bound).astype(kind)


def setup_inputs(seed: int = 0, part: int = 0) -> dict:
    streams_of = jax.random.split(jax.random.key(seed), 15)
    part_keys = jax.random.split(jax.random.fold_in(streams_of[14], part), 15)
    return {
        "tokens": gaussian(part_keys[0], (SEQ, D), 1.0, 6.0, ((0, 4),)),
        "chosen": draw_chosen(jax.random.fold_in(jax.random.fold_in(streams_of[14], part), 71), part),
        "w_query": gaussian(streams_of[2], (D, HEADS * HEAD), D ** -0.5, 0.1875, ((1, 2),)),
        "w_key_summary": gaussian(streams_of[3], (D, GROUPS * HEAD), D ** -0.5, 0.1875),
        "w_value_summary": gaussian(streams_of[4], (D, GROUPS * HEAD), D ** -0.5, 0.1875),
        "w_key_chosen": gaussian(streams_of[5], (D, GROUPS * HEAD), D ** -0.5, 0.1875),
        "w_value_chosen": gaussian(streams_of[6], (D, GROUPS * HEAD), D ** -0.5, 0.1875),
        "squeeze_key_in": gaussian(streams_of[7], (CMP_LEN * HEAD, HEAD), (CMP_LEN * HEAD) ** -0.5, 0.125),
        "squeeze_key_out": gaussian(streams_of[8], (HEAD, HEAD), HEAD ** -0.5, 0.75),
        "squeeze_value_in": gaussian(streams_of[9], (CMP_LEN * HEAD, HEAD), (CMP_LEN * HEAD) ** -0.5, 0.125),
        "squeeze_value_out": gaussian(streams_of[10], (HEAD, HEAD), HEAD ** -0.5, 0.75),
        "w_gates": gaussian(streams_of[11], (D, 2 * HEADS), D ** -0.5, 0.1875),
        "w_out": gaussian(streams_of[12], (HEADS * HEAD, D), (HEADS * HEAD) ** -0.5, 0.25),
        "out_gain": jnp.clip(1.0 + 0.18 * jax.random.normal(streams_of[13], (D,), jnp.float32), 0.1, 1.9),
    }


EPS = 1e-06

def project(tokens, weight):
    return jnp.dot(tokens, weight, preferred_element_type=jnp.float32).astype(jnp.bfloat16)

def squeeze(rows, w_in, w_out):
    feature_width = rows.shape[1]
    block_count = rows.shape[0] // CMP_STRIDE
    padded = jnp.concatenate([rows, jnp.zeros((CMP_STRIDE, feature_width), jnp.bfloat16)], axis=0)
    halves = padded.reshape(block_count + 1, CMP_STRIDE, feature_width)
    joined = jnp.concatenate([halves[:-1], halves[1:]], axis=1).reshape(block_count, CMP_LEN * feature_width)
    hidden = jax.nn.gelu(jnp.dot(joined, w_in, preferred_element_type=jnp.float32)).astype(jnp.bfloat16)
    return jnp.dot(hidden, w_out, preferred_element_type=jnp.float32).astype(jnp.bfloat16)

def rounded(weights):
    return lax.optimization_barrier(weights.astype(jnp.bfloat16)).astype(jnp.float32)

def finish(weighted, weight_sum):
    denom = jnp.where(weight_sum > 0, weight_sum, 1.0)
    return weighted / denom[..., None]

def reference(tokens, chosen, w_query, w_key_summary, w_value_summary, w_key_chosen, w_value_chosen, squeeze_key_in, squeeze_key_out, squeeze_value_in, squeeze_value_out, w_gates, w_out, out_gain):
    per_group = HEADS // GROUPS
    score_scale = HEAD ** (-0.5)
    queries = project(tokens, w_query).reshape(SEQ, GROUPS, per_group, HEAD).astype(jnp.float32)
    key_raw = project(tokens, w_key_summary).reshape(SEQ, GROUPS, HEAD)
    value_raw = project(tokens, w_value_summary).reshape(SEQ, GROUPS, HEAD)
    key_sum = jnp.stack([squeeze(key_raw[:, group_index], squeeze_key_in, squeeze_key_out) for group_index in range(GROUPS)]).astype(jnp.float32)
    value_sum = jnp.stack([squeeze(value_raw[:, group_index], squeeze_value_in, squeeze_value_out) for group_index in range(GROUPS)]).astype(jnp.float32)
    key_pick = project(tokens, w_key_chosen).reshape(SEGMENT_TALLY, SEL, GROUPS, HEAD).transpose(2, 0, 1, 3).astype(jnp.float32)
    value_pick = project(tokens, w_value_chosen).reshape(SEGMENT_TALLY, SEL, GROUPS, HEAD).transpose(2, 0, 1, 3).astype(jnp.float32)
    summary_ends = (jnp.arange(key_sum.shape[1]) * CMP_STRIDE + CMP_LEN - 1).astype(jnp.int32)
    group_rows = jnp.arange(GROUPS).astype(jnp.int32)[:, None]
    offsets = jnp.arange(SEL).astype(jnp.int32)

    def one_block(block_index):
        first_pos = (block_index * SEL).astype(jnp.int32)
        q_block = lax.dynamic_slice_in_dim(queries, first_pos, SEL, 0)
        positions = first_pos + offsets
        scores = jnp.einsum('qgrd,gcd->qgrc', q_block, key_sum) * score_scale
        visible = (summary_ends[None, :] <= positions[:, None])[:, None, None, :]
        masked = jnp.where(visible, scores, -1e+30)
        peak_score = lax.optimization_barrier(jnp.max(masked, axis=-1, keepdims=True))
        weights = jnp.where(visible, jnp.exp(masked - peak_score), 0.0)
        weighted = jnp.einsum('qgrc,gcd->qgrd', rounded(weights), value_sum)
        summary_out = finish(weighted, lax.optimization_barrier(jnp.sum(weights, axis=-1)))
        picked = chosen[block_index].astype(jnp.int32)
        key_blocks = key_pick[group_rows, picked]
        value_blocks = value_pick[group_rows, picked]
        pick_scores = jnp.einsum('qgrd,gksd->qgrks', q_block, key_blocks) * score_scale
        key_places = picked[:, :, None] * SEL + offsets[None, None, :]
        pick_visible = key_places[None, :, None, :, :] <= positions[:, None, None, None, None]
        pick_masked = jnp.where(pick_visible, pick_scores, -1e+30)
        pick_peak = lax.optimization_barrier(jnp.max(pick_masked, axis=(-2, -1), keepdims=True))
        pick_weights = jnp.where(pick_visible, jnp.exp(pick_masked - pick_peak), 0.0)
        pick_weighted = jnp.einsum('qgrks,gksd->qgrd', rounded(pick_weights), value_blocks)
        chosen_out = finish(pick_weighted, lax.optimization_barrier(jnp.sum(pick_weights, axis=(-2, -1))))
        return (summary_out, chosen_out)
    summary_out, chosen_out = lax.map(one_block, jnp.arange(SEGMENT_TALLY))
    summary_out = summary_out.reshape(SEQ, HEADS, HEAD)
    chosen_out = chosen_out.reshape(SEQ, HEADS, HEAD)
    gate_values = jax.nn.sigmoid(jnp.dot(tokens, w_gates, preferred_element_type=jnp.float32)).reshape(SEQ, HEADS, 2)
    mixed_heads = (gate_values[..., 0:1] * summary_out + gate_values[..., 1:2] * chosen_out).astype(jnp.bfloat16)
    projected = jnp.dot(mixed_heads.reshape(SEQ, HEADS * HEAD), w_out, preferred_element_type=jnp.float32)
    row_power = lax.optimization_barrier(jnp.mean(projected * projected, axis=-1, keepdims=True))
    return (projected * lax.rsqrt(row_power + EPS) * out_gain).astype(jnp.bfloat16)
```

```python
import functools

import jax
import jax.numpy as jnp
from jax import lax
from jax.experimental import pallas as pl
from jax.experimental.pallas import tpu as pltpu
from jax.sharding import PartitionSpec as P

HEAD = 64
CMP_STRIDE = 16
CMP_LEN = 32
SEL = 64
LANES = 128
EPS = 1e-06
NEG = -1e30
MESH = pl.DeviceIdType.MESH
F32 = jnp.float32
BF16 = jnp.bfloat16


def dot(a, b):
    return jnp.dot(a, b, preferred_element_type=F32)


def dot_t(a, b):
    return lax.dot_general(a, b, (((1,), (1,)), ((), ())), preferred_element_type=F32)


def swap(x):
    return pltpu.roll(x, HEAD, 1)


def low_lanes(shape):
    return lax.broadcasted_iota(jnp.int32, shape, 1) < HEAD


def kernel(
    spans,
    tokens_h,
    chosen_ref,
    wq_h,
    wks_h,
    wvs_h,
    wkc_h,
    wvc_h,
    ski_h,
    sko_h,
    svi_h,
    svo_h,
    wg_h,
    wo_h,
    gain_ref,
    out_ref,
    tokens,
    wq,
    wsum,
    wcho,
    ski,
    sko,
    svi,
    svo,
    wg,
    wo,
    raw,
    kv_all,
    pre_all,
    sum_kv,
    q_s,
    gates,
    bias,
    acc,
    m_s,
    l_s,
    mixed_own,
    mixed_other,
    in_sem,
    kv_send,
    kv_recv,
    pre_send,
    pre_recv,
    mix_send,
    mix_recv,
):
    me = lax.axis_index("kv")
    group = lax.axis_index("tp")
    first = group == 0
    rows, _ = tokens.shape
    blocks = rows // SEL
    cmp_rows = rows // CMP_STRIDE
    heads = wq.shape[1] // HEAD
    q_rows = heads * SEL

    loads = [
        pltpu.make_async_copy(src, dst, in_sem.at[i])
        for i, (src, dst) in enumerate(
            [
                (wks_h, wsum.at[:, pl.ds(0, LANES)]),
                (wvs_h, wsum.at[:, pl.ds(LANES, LANES)]),
                (wkc_h, wcho.at[:, pl.ds(0, LANES)]),
                (wvc_h, wcho.at[:, pl.ds(LANES, LANES)]),
                (tokens_h, tokens),
                (ski_h, ski),
                (svi_h, svi),
                (wq_h, wq),
                (wg_h, wg),
                (sko_h, sko),
                (svo_h, svo),
                (wo_h, wo),
            ]
        )
    ]
    for load in loads:
        load.start()

    barrier = pltpu.get_barrier_semaphore()

    def greet(step, carry):
        other = lax.rem(me + step, spans)
        pl.semaphore_signal(barrier, inc=1, device_id={"kv": other}, device_id_type=MESH)
        return carry

    lax.fori_loop(1, spans, greet, 0)
    pl.semaphore_signal(barrier, inc=1, device_id={"tp": 1 - group}, device_id_type=MESH)

    for load in loads[:5]:
        load.wait()
    low = low_lanes((rows, LANES))

    def pair(both):
        k2, v2 = both[:, :LANES], both[:, LANES:]
        k_side = jnp.where(first, k2, swap(k2))
        v_side = jnp.where(first, swap(v2), v2)
        return jnp.where(low, k_side, v_side)

    raw[...] = pair(dot(tokens[...], wsum[...]))
    kv_all[me] = pair(dot(tokens[...], wcho[...])).astype(BF16)

    for load in loads[5:7]:
        load.wait()
    low_c = low_lanes((cmp_rows, LANES))
    key_tiles, value_tiles = [], []
    for a in range(CMP_STRIDE // 2):
        even = raw[pl.ds(2 * a, cmp_rows, stride=CMP_STRIDE), :]
        odd = raw[pl.ds(2 * a + 1, cmp_rows, stride=CMP_STRIDE), :]
        key_tiles.append(jnp.where(low_c, even, swap(odd)).astype(BF16))
        value_tiles.append(jnp.where(low_c, swap(even), odd).astype(BF16))
    half = CMP_STRIDE * HEAD
    joined_k = jnp.concatenate(key_tiles, axis=1)
    joined_v = jnp.concatenate(value_tiles, axis=1)
    head_sum = jnp.concatenate(
        [dot(joined_k, ski[pl.ds(0, half), :]), dot(joined_v, svi[pl.ds(0, half), :])], axis=1
    )
    tail_sum = jnp.concatenate(
        [dot(joined_k, ski[pl.ds(half, half), :]), dot(joined_v, svi[pl.ds(half, half), :])], axis=1
    )
    row_c = lax.broadcasted_iota(jnp.int32, (cmp_rows, LANES), 0)
    shifted = jnp.where(row_c < cmp_rows - 1, pltpu.roll(tail_sum, cmp_rows - 1, 0), 0.0)
    pre_all[me, pl.ds(0, cmp_rows), :] = head_sum + shifted
    pre_all[me, pl.ds(cmp_rows, 8), :] = tail_sum[:8]

    def clear(span, carry):
        pre_all[span] = jnp.zeros(pre_all.shape[1:], F32)
        return carry

    lax.fori_loop(me + 1, spans, clear, 0)

    pl.semaphore_wait(barrier, spans)

    def pre_copy(source, target):
        return pltpu.make_async_remote_copy(
            src_ref=pre_all.at[source],
            dst_ref=pre_all.at[source],
            send_sem=pre_send.at[target],
            recv_sem=pre_recv.at[source],
            device_id={"kv": target},
            device_id_type=MESH,
        )

    def kv_copy(source, target):
        return pltpu.make_async_remote_copy(
            src_ref=kv_all.at[source],
            dst_ref=kv_all.at[source],
            send_sem=kv_send.at[target],
            recv_sem=kv_recv.at[source],
            device_id={"kv": target},
            device_id_type=MESH,
        )

    def send_pre(step, carry):
        pre_copy(me, spans - 1 - step).start()
        return carry

    def send_kv(step, carry):
        kv_copy(me, spans - 1 - step).start()
        return carry

    lax.fori_loop(0, spans - 1 - me, send_pre, 0)
    lax.fori_loop(0, spans - 1 - me, send_kv, 0)

    for load in loads[7:9]:
        load.wait()
    scaled = dot(tokens[...], wq[...]).astype(BF16).astype(F32) * (HEAD**-0.5)
    for a in range(heads // 2):
        tile = scaled[:, a * LANES : (a + 1) * LANES]
        even = jnp.where(low, tile, 0.0).astype(BF16)
        odd = jnp.where(low, swap(tile), 0.0).astype(BF16)
        q_s[:, pl.ds(2 * a * SEL, SEL), :] = even.reshape(blocks, SEL, LANES)
        q_s[:, pl.ds((2 * a + 1) * SEL, SEL), :] = odd.reshape(blocks, SEL, LANES)
    gate_all = jax.nn.sigmoid(dot(tokens[...], wg[...]))
    width = 2 * heads
    gates[...] = jnp.where(first, gate_all[:, :width], gate_all[:, width : 2 * width])

    def set_bias(span):
        ids = span * blocks + lax.broadcasted_iota(jnp.int32, (blocks, rows), 1) // SEL
        picks = chosen_ref[:, 0, :]
        hit = jnp.zeros((blocks, rows), F32)
        for t in range(picks.shape[1]):
            hit = jnp.where(picks[:, t : t + 1] == ids, 1.0, hit)
        bias[...] = jnp.where(hit > 0.0, 0.0, NEG)

    def lane_sum(p):
        total = p[:, :LANES]
        for c in range(1, p.shape[1] // LANES):
            total = total + p[:, c * LANES : (c + 1) * LANES]
        return total

    set_bias(me)

    def own_block(j, carry):
        keys = kv_all[me]
        scores = dot_t(q_s[j], keys) + bias[pl.ds(j, 1), :]
        place = lax.broadcasted_iota(jnp.int32, scores.shape, 1)
        time = j * SEL + lax.broadcasted_iota(jnp.int32, scores.shape, 0) % SEL
        scores = jnp.where(place <= time, scores, NEG)
        peak = jnp.max(scores, axis=1, keepdims=True)
        p = jnp.exp(scores - peak)
        m_s[j] = jnp.broadcast_to(peak, (q_rows, LANES))
        l_s[j] = lane_sum(p)
        acc[j] = dot(p.astype(BF16), keys)
        return carry

    lax.fori_loop(0, blocks, own_block, 0)

    def span_step(step, carry):
        span = me - 1 - step
        set_bias(span)
        kv_copy(span, me).wait_recv()

        def block(j, inner):
            keys = kv_all[span]
            scores = dot_t(q_s[j], keys) + bias[pl.ds(j, 1), :]
            old = m_s[j]
            peak = jnp.maximum(old, jnp.max(scores, axis=1, keepdims=True))
            p = jnp.exp(scores - peak[:, :1])
            fix = jnp.exp(old - peak)
            m_s[j] = peak
            l_s[j] = l_s[j] * fix + lane_sum(p)
            acc[j] = acc[j] * fix + dot(p.astype(BF16), keys)
            return inner

        return lax.fori_loop(0, blocks, block, carry)

    lax.fori_loop(0, me, span_step, 0)

    def await_pre(span, carry):
        pre_copy(span, me).wait_recv()
        return carry

    lax.fori_loop(0, me, await_pre, 0)
    for load in loads[9:11]:
        load.wait()
    parts = []
    for span in range(spans):
        part = pre_all[span, pl.ds(0, cmp_rows), :]
        if span + 1 < spans:
            part = part + jnp.where(
                row_c == cmp_rows - 1, pre_all[span + 1, pl.ds(cmp_rows, 1), :], 0.0
            )
        parts.append(part)
    hidden = jax.nn.gelu(jnp.concatenate(parts, axis=0)).astype(BF16)
    sum_kv[...] = jnp.concatenate(
        [dot(hidden[:, :HEAD], sko[...]), dot(hidden[:, HEAD:], svo[...])], axis=1
    ).astype(BF16)

    low_q = low_lanes((SEL, LANES))

    def mix_copy(j):
        part = pl.ds(pl.multiple_of(j * SEL, SEL), SEL)
        return pltpu.make_async_remote_copy(
            src_ref=mixed_own.at[part, :],
            dst_ref=mixed_other.at[part, :],
            send_sem=mix_send.at[j],
            recv_sem=mix_recv.at[j],
            device_id={"tp": 1 - group},
            device_id_type=MESH,
        )

    def finish_block(j, carry):
        table = sum_kv[...]
        scores = dot_t(q_s[j], table)
        ends = lax.broadcasted_iota(jnp.int32, scores.shape, 1) * CMP_STRIDE + CMP_LEN - 1
        time = me * rows + j * SEL + lax.broadcasted_iota(jnp.int32, scores.shape, 0) % SEL
        visible = ends <= time
        scores = jnp.where(visible, scores, NEG)
        peak = jnp.max(scores, axis=1, keepdims=True)
        p = jnp.where(visible, jnp.exp(scores - peak), 0.0)
        weight = jnp.sum(p, axis=1, keepdims=True)
        summary = dot(p.astype(BF16), table) / jnp.where(weight > 0.0, weight, 1.0)
        picked = acc[j] / jnp.sum(l_s[j], axis=1, keepdims=True)
        part = pl.ds(pl.multiple_of(j * SEL, SEL), SEL)
        gate = gates[part, :]
        heads_out = []
        for h in range(heads):
            cut = slice(h * SEL, (h + 1) * SEL)
            heads_out.append(
                gate[:, 2 * h : 2 * h + 1] * summary[cut] + gate[:, 2 * h + 1 : 2 * h + 2] * picked[cut]
            )
        tiles = [
            jnp.where(low_q, swap(heads_out[2 * a]), heads_out[2 * a + 1]) for a in range(heads // 2)
        ]
        mixed_own[part, :] = jnp.concatenate(tiles, axis=1).astype(BF16)
        mix_copy(j).start()
        return carry

    lax.fori_loop(0, blocks, finish_block, 0)
    loads[11].wait()

    half_rows = heads * HEAD
    half_cols = wo.shape[1] // 2
    own_rows = pl.ds(pl.multiple_of(group * half_rows, half_rows), half_rows)
    other_rows = pl.ds(pl.multiple_of((1 - group) * half_rows, half_rows), half_rows)
    own_cols = pl.ds(pl.multiple_of(group * half_cols, half_cols), half_cols)
    other_cols = pl.ds(pl.multiple_of((1 - group) * half_cols, half_cols), half_cols)

    def project_block(j, carry):
        for b in range(2):
            mix_copy(2 * j + b).wait_recv()
        part = pl.ds(pl.multiple_of(2 * j * SEL, 2 * SEL), 2 * SEL)
        own, other = mixed_own[part, :], mixed_other[part, :]
        mine = dot(own, wo[own_rows, own_cols]) + dot(other, wo[other_rows, own_cols])
        rest = dot(own, wo[own_rows, other_cols]) + dot(other, wo[other_rows, other_cols])
        power = jnp.sum(mine * mine + rest * rest, axis=1, keepdims=True)
        scale = lax.rsqrt(power / wo.shape[1] + EPS)
        out_ref[part, :] = (mine * scale * gain_ref[:, own_cols]).astype(BF16)
        return carry

    lax.fori_loop(0, blocks // 2, project_block, 0)

    def end_mix(j, carry):
        mix_copy(j).wait_send()
        return carry

    lax.fori_loop(0, blocks, end_mix, 0)

    def end_sends(step, carry):
        pre_copy(me, spans - 1 - step).wait_send()
        kv_copy(me, spans - 1 - step).wait_send()
        return carry

    lax.fori_loop(0, spans - 1 - me, end_sends, 0)


def local(spans, tokens, chosen, *weights):
    w_query, w_ks, w_vs, w_kc, w_vc, ski, sko, svi, svo, w_gates, w_out, gain = weights
    rows, width = tokens.shape
    heads = w_query.shape[1] // HEAD
    blocks = rows // SEL
    cmp_rows = rows // CMP_STRIDE
    any_spec = pl.BlockSpec(memory_space=pl.ANY)
    vmem = pl.BlockSpec(memory_space=pltpu.VMEM)
    dma = pltpu.SemaphoreType.DMA
    return pl.pallas_call(
        functools.partial(kernel, spans),
        out_shape=jax.ShapeDtypeStruct((rows, w_out.shape[1] // 2), BF16),
        in_specs=[any_spec, vmem] + [any_spec] * 11 + [vmem],
        out_specs=vmem,
        scratch_shapes=[
            pltpu.VMEM(tokens.shape, BF16),
            pltpu.VMEM(w_query.shape, BF16),
            pltpu.VMEM((width, 2 * w_ks.shape[1]), BF16),
            pltpu.VMEM((width, 2 * w_kc.shape[1]), BF16),
            pltpu.VMEM(ski.shape, BF16),
            pltpu.VMEM(sko.shape, BF16),
            pltpu.VMEM(svi.shape, BF16),
            pltpu.VMEM(svo.shape, BF16),
            pltpu.VMEM(w_gates.shape, BF16),
            pltpu.VMEM(w_out.shape, BF16),
            pltpu.VMEM((rows, LANES), F32),
            pltpu.VMEM((spans, rows, LANES), BF16),
            pltpu.VMEM((spans, cmp_rows + 8, LANES), F32),
            pltpu.VMEM((spans * cmp_rows, LANES), BF16),
            pltpu.VMEM((blocks, heads * SEL, LANES), BF16),
            pltpu.VMEM((rows, 2 * heads), F32),
            pltpu.VMEM((blocks, rows), F32),
            pltpu.VMEM((blocks, heads * SEL, LANES), F32),
            pltpu.VMEM((blocks, heads * SEL, LANES), F32),
            pltpu.VMEM((blocks, heads * SEL, LANES), F32),
            pltpu.VMEM((rows, heads * HEAD), BF16),
            pltpu.VMEM((rows, heads * HEAD), BF16),
            dma((12,)),
            dma((spans,)),
            dma((spans,)),
            dma((spans,)),
            dma((spans,)),
            dma((blocks,)),
            dma((blocks,)),
        ],
        compiler_params=pltpu.CompilerParams(collective_id=0, has_side_effects=True),
    )(
        tokens,
        chosen,
        w_query,
        w_ks,
        w_vs,
        w_kc,
        w_vc,
        ski,
        sko,
        svi,
        svo,
        w_gates,
        w_out,
        gain.reshape(1, -1),
    )


def solution(mesh):
    in_specs = (
        P(("dp", "kv"), None),
        P(("dp", "kv"), "tp", None),
        P(None, "tp"),
    ) + (P(),) * 11
    return jax.shard_map(
        functools.partial(local, mesh.shape["kv"]),
        mesh=mesh,
        in_specs=in_specs,
        out_specs=P(("dp", "kv"), "tp"),
        check_vma=False,
    )
```

```python
import functools

import jax
import jax.numpy as jnp
from jax import lax
from jax.experimental import pallas as pl
from jax.experimental.pallas import tpu as pltpu
from jax.sharding import PartitionSpec as P

HEAD = 64
CMP_STRIDE = 16
CMP_LEN = 32
SEL = 64
CAP = 4
LANES = 128
EPS = 1e-06
NEG = -1e30
MESH = pl.DeviceIdType.MESH
F32 = jnp.float32
BF16 = jnp.bfloat16


def dot(a, b):
    return jnp.dot(a, b, preferred_element_type=F32)


def dot_t(a, b):
    return lax.dot_general(a, b, (((1,), (1,)), ((), ())), preferred_element_type=F32)


def swap(x):
    return pltpu.roll(x, HEAD, 1)


def low_lanes(shape):
    return lax.broadcasted_iota(jnp.int32, shape, 1) < HEAD


def kernel(
    spans,
    tokens_h,
    chosen_ref,
    wq_h,
    wks_h,
    wvs_h,
    wkc_h,
    wvc_h,
    ski_h,
    sko_h,
    svi_h,
    svo_h,
    wg_h,
    wo_h,
    gain_ref,
    out_ref,
    tokens,
    wq,
    wsum,
    wcho,
    ski,
    sko,
    svi,
    svo,
    wg,
    wo,
    raw,
    kv_own,
    kv_all,
    packed,
    asks,
    slots,
    pre_all,
    sum_kv,
    q_s,
    gates,
    bias,
    far_bias,
    acc,
    m_s,
    l_s,
    mixed_own,
    mixed_other,
    in_sem,
    ask_send,
    ask_recv,
    kv_send,
    kv_recv,
    pre_send,
    pre_recv,
    mix_send,
    mix_recv,
):
    me = lax.axis_index("kv")
    group = lax.axis_index("tp")
    first = group == 0
    rows, _ = tokens.shape
    blocks = rows // SEL
    cmp_rows = rows // CMP_STRIDE
    heads = wq.shape[1] // HEAD
    q_rows = heads * SEL

    loads = [
        pltpu.make_async_copy(src, dst, in_sem.at[i])
        for i, (src, dst) in enumerate(
            [
                (wkc_h, wcho.at[:, pl.ds(0, LANES)]),
                (wvc_h, wcho.at[:, pl.ds(LANES, LANES)]),
                (tokens_h, tokens),
                (wks_h, wsum.at[:, pl.ds(0, LANES)]),
                (wvs_h, wsum.at[:, pl.ds(LANES, LANES)]),
                (ski_h, ski),
                (svi_h, svi),
                (wq_h, wq),
                (wg_h, wg),
                (sko_h, sko),
                (svo_h, svo),
                (wo_h, wo),
            ]
        )
    ]
    for load in loads:
        load.start()

    barrier = pltpu.get_barrier_semaphore()

    def greet(step, carry):
        other = lax.rem(me + step, spans)
        pl.semaphore_signal(barrier, inc=1, device_id={"kv": other}, device_id_type=MESH)
        return carry

    lax.fori_loop(1, spans, greet, 0)
    pl.semaphore_signal(barrier, inc=1, device_id={"tp": 1 - group}, device_id_type=MESH)

    low = low_lanes((rows, LANES))

    def ask_copy(source, target):
        return pltpu.make_async_remote_copy(
            src_ref=chosen_ref,
            dst_ref=asks.at[source],
            send_sem=ask_send.at[target],
            recv_sem=ask_recv.at[source],
            device_id={"kv": target},
            device_id_type=MESH,
        )

    def kv_copy(source, target):
        return pltpu.make_async_remote_copy(
            src_ref=packed.at[target],
            dst_ref=kv_all.at[source],
            send_sem=kv_send.at[target],
            recv_sem=kv_recv.at[source],
            device_id={"kv": target},
            device_id_type=MESH,
        )

    pl.semaphore_wait(barrier, spans)

    def send_ask(span, carry):
        ask_copy(me, span).start()
        return carry

    lax.fori_loop(0, me, send_ask, 0)

    def block_of_slot(picks):
        lanes = -(-spans * blocks // LANES) * LANES
        ids = lax.broadcasted_iota(jnp.int32, (blocks, lanes), 1)
        hit = jnp.zeros((blocks, lanes), jnp.int32)
        for t in range(picks.shape[1]):
            hit = jnp.where(picks[:, t : t + 1] == ids, 1, hit)
        need = jnp.broadcast_to(jnp.max(hit, axis=0, keepdims=True), (8, lanes))
        lane = lax.broadcasted_iota(jnp.int32, (8, lanes), 1)
        rank = jnp.zeros((8, lanes), jnp.int32)
        for d in range(1, blocks):
            rank = rank + jnp.where(lane % blocks >= d, pltpu.roll(need, d, 1), 0)
        code = jnp.where((need > 0) & (rank < CAP), lane // blocks * CAP + rank, -1)[:1]
        place = lax.broadcasted_iota(jnp.int32, (spans * CAP, lanes), 0)
        id_row = lax.broadcasted_iota(jnp.int32, (spans * CAP, lanes), 1)
        found = jnp.where(code == place, id_row, -1)
        return jnp.broadcast_to(jnp.max(found, axis=1, keepdims=True), (spans * CAP, LANES))

    def pair(both):
        k2, v2 = both[:, :LANES], both[:, LANES:]
        k_side = jnp.where(first, k2, swap(k2))
        v_side = jnp.where(first, swap(v2), v2)
        return jnp.where(low, k_side, v_side)

    for load in loads[:3]:
        load.wait()
    kv_own[...] = pair(dot(tokens[...], wcho[...])).astype(BF16)

    def serve(step, carry):
        target = spans - 1 - step
        ask_copy(target, me).wait_recv()
        slots[...] = block_of_slot(asks[target][:, 0, :])
        key_lane = lax.broadcasted_iota(jnp.int32, (SEL, rows), 1)
        key_row = lax.broadcasted_iota(jnp.int32, (SEL, rows), 0)
        ours = slots[pl.ds(me * CAP, CAP), :]
        pieces = []
        for k in range(CAP):
            start = (ours[k : k + 1, :1] - me * blocks) * SEL
            pieces.append(jnp.where(key_lane == start + key_row, 1.0, 0.0).astype(BF16))
        packed[target] = dot(jnp.concatenate(pieces, axis=0), kv_own[...]).astype(BF16)
        kv_copy(me, target).start()
        return carry

    lax.fori_loop(0, spans - 1 - me, serve, 0)

    for load in loads[3:5]:
        load.wait()
    raw[...] = pair(dot(tokens[...], wsum[...]))

    for load in loads[5:7]:
        load.wait()
    low_c = low_lanes((cmp_rows, LANES))
    key_tiles, value_tiles = [], []
    for a in range(CMP_STRIDE // 2):
        even = raw[pl.ds(2 * a, cmp_rows, stride=CMP_STRIDE), :]
        odd = raw[pl.ds(2 * a + 1, cmp_rows, stride=CMP_STRIDE), :]
        key_tiles.append(jnp.where(low_c, even, swap(odd)).astype(BF16))
        value_tiles.append(jnp.where(low_c, swap(even), odd).astype(BF16))
    half = CMP_STRIDE * HEAD
    joined_k = jnp.concatenate(key_tiles, axis=1)
    joined_v = jnp.concatenate(value_tiles, axis=1)
    head_sum = jnp.concatenate(
        [dot_t(joined_k, ski[:, pl.ds(0, half)]), dot_t(joined_v, svi[:, pl.ds(0, half)])], axis=1
    )
    tail_sum = jnp.concatenate(
        [dot_t(joined_k, ski[:, pl.ds(half, half)]), dot_t(joined_v, svi[:, pl.ds(half, half)])], axis=1
    )
    row_c = lax.broadcasted_iota(jnp.int32, (cmp_rows, LANES), 0)
    shifted = jnp.where(row_c < cmp_rows - 1, pltpu.roll(tail_sum, cmp_rows - 1, 0), 0.0)
    pre_all[me, pl.ds(0, cmp_rows), :] = head_sum + shifted
    pre_all[me, pl.ds(cmp_rows, 8), :] = tail_sum[:8]

    def clear(span, carry):
        pre_all[span] = jnp.zeros(pre_all.shape[1:], F32)
        return carry

    lax.fori_loop(me + 1, spans, clear, 0)

    def pre_copy(source, target):
        return pltpu.make_async_remote_copy(
            src_ref=pre_all.at[source],
            dst_ref=pre_all.at[source],
            send_sem=pre_send.at[target],
            recv_sem=pre_recv.at[source],
            device_id={"kv": target},
            device_id_type=MESH,
        )

    def send_pre(step, carry):
        pre_copy(me, spans - 1 - step).start()
        return carry

    lax.fori_loop(0, spans - 1 - me, send_pre, 0)

    for load in loads[7:9]:
        load.wait()
    scaled = dot(tokens[...], wq[...]).astype(BF16).astype(F32) * (HEAD**-0.5)
    for a in range(heads // 2):
        tile = scaled[:, a * LANES : (a + 1) * LANES]
        even = jnp.where(low, tile, 0.0).astype(BF16)
        odd = jnp.where(low, swap(tile), 0.0).astype(BF16)
        q_s[:, pl.ds(2 * a * SEL, SEL), :] = even.reshape(blocks, SEL, LANES)
        q_s[:, pl.ds((2 * a + 1) * SEL, SEL), :] = odd.reshape(blocks, SEL, LANES)
    gate_all = jax.nn.sigmoid(dot_t(tokens[...], wg[...]))
    width = 2 * heads
    gates[...] = jnp.where(first, gate_all[:, :width], gate_all[:, width : 2 * width])

    picks = chosen_ref[:, 0, :]

    def bias_of(ids):
        hit = jnp.zeros((blocks, ids.shape[1]), F32)
        for t in range(picks.shape[1]):
            hit = jnp.where(picks[:, t : t + 1] == ids, 1.0, hit)
        return jnp.where(hit > 0.0, 0.0, NEG)

    def lane_sum(p):
        total = p[:, :LANES]
        for c in range(1, p.shape[1] // LANES):
            total = total + p[:, c * LANES : (c + 1) * LANES]
        return total

    bias[...] = bias_of(me * blocks + lax.broadcasted_iota(jnp.int32, (blocks, rows), 1) // SEL)
    slots[...] = block_of_slot(picks)
    low_b = low_lanes((blocks, LANES))

    def set_bias(span, carry):
        ids = slots[pl.ds(span * CAP, CAP), :]
        tiles = [
            jnp.where(low_b, ids[2 * a : 2 * a + 1], ids[2 * a + 1 : 2 * a + 2])
            for a in range(CAP // 2)
        ]
        far_bias[span] = bias_of(jnp.concatenate(tiles, axis=1))
        return carry

    lax.fori_loop(0, me, set_bias, 0)

    def own_values(j):
        keys = kv_own[...]
        scores = dot_t(q_s[j], keys) + bias[pl.ds(j, 1), :]
        place = lax.broadcasted_iota(jnp.int32, scores.shape, 1)
        time = j * SEL + lax.broadcasted_iota(jnp.int32, scores.shape, 0) % SEL
        scores = jnp.where(place <= time, scores, NEG)
        peak = jnp.max(scores, axis=1, keepdims=True)
        p = jnp.exp(scores - peak)
        return jnp.broadcast_to(peak, (q_rows, LANES)), lane_sum(p), dot(p.astype(BF16), keys)

    def in_pairs(values):
        def step(jj, carry):
            both = (2 * jj, 2 * jj + 1)
            for j, (peak, weight, total) in zip(both, [values(j) for j in both]):
                m_s[j] = peak
                l_s[j] = weight
                acc[j] = total
            return carry

        lax.fori_loop(0, blocks // 2, step, 0)

    in_pairs(own_values)

    def span_step(step, carry):
        span = me - 1 - step
        kv_copy(span, me).wait_recv()

        def far_values(j):
            keys = kv_all[span]
            scores = dot_t(q_s[j], keys) + far_bias[span, pl.ds(j, 1), :]
            old = m_s[j]
            peak = jnp.maximum(old, jnp.max(scores, axis=1, keepdims=True))
            p = jnp.exp(scores - peak[:, :1])
            fix = jnp.exp(old - peak)
            return peak, l_s[j] * fix + lane_sum(p), acc[j] * fix + dot(p.astype(BF16), keys)

        in_pairs(far_values)
        return carry

    lax.fori_loop(0, me, span_step, 0)

    def await_pre(span, carry):
        pre_copy(span, me).wait_recv()
        return carry

    lax.fori_loop(0, me, await_pre, 0)
    for load in loads[9:11]:
        load.wait()
    parts = []
    for span in range(spans):
        part = pre_all[span, pl.ds(0, cmp_rows), :]
        if span + 1 < spans:
            part = part + jnp.where(
                row_c == cmp_rows - 1, pre_all[span + 1, pl.ds(cmp_rows, 1), :], 0.0
            )
        parts.append(part)
    hidden = jax.nn.gelu(jnp.concatenate(parts, axis=0)).astype(BF16)
    sum_kv[...] = jnp.concatenate(
        [dot(hidden[:, :HEAD], sko[...]), dot(hidden[:, HEAD:], svo[...])], axis=1
    ).astype(BF16)

    low_q = low_lanes((SEL, LANES))

    def mix_copy(j):
        part = pl.ds(pl.multiple_of(j * SEL, SEL), SEL)
        return pltpu.make_async_remote_copy(
            src_ref=mixed_own.at[part, :],
            dst_ref=mixed_other.at[part, :],
            send_sem=mix_send.at[j],
            recv_sem=mix_recv.at[j],
            device_id={"tp": 1 - group},
            device_id_type=MESH,
        )

    def finished(j):
        table = sum_kv[...]
        scores = dot_t(q_s[j], table)
        ends = lax.broadcasted_iota(jnp.int32, scores.shape, 1) * CMP_STRIDE + CMP_LEN - 1
        time = me * rows + j * SEL + lax.broadcasted_iota(jnp.int32, scores.shape, 0) % SEL
        visible = ends <= time
        scores = jnp.where(visible, scores, NEG)
        peak = jnp.max(scores, axis=1, keepdims=True)
        p = jnp.where(visible, jnp.exp(scores - peak), 0.0)
        weight = jnp.sum(p, axis=1, keepdims=True)
        summary = dot(p.astype(BF16), table) / jnp.where(weight > 0.0, weight, 1.0)
        picked = acc[j] / jnp.sum(l_s[j], axis=1, keepdims=True)
        part = pl.ds(pl.multiple_of(j * SEL, SEL), SEL)
        gate = gates[part, :]
        heads_out = []
        for h in range(heads):
            cut = slice(h * SEL, (h + 1) * SEL)
            heads_out.append(
                gate[:, 2 * h : 2 * h + 1] * summary[cut] + gate[:, 2 * h + 1 : 2 * h + 2] * picked[cut]
            )
        tiles = [
            jnp.where(low_q, swap(heads_out[2 * a]), heads_out[2 * a + 1]) for a in range(heads // 2)
        ]
        return part, jnp.concatenate(tiles, axis=1).astype(BF16)

    def finish_pair(jj, carry):
        both = (2 * jj, 2 * jj + 1)
        for part, mixed in [finished(j) for j in both]:
            mixed_own[part, :] = mixed
        for j in both:
            mix_copy(j).start()
        return carry

    lax.fori_loop(0, blocks // 2, finish_pair, 0)
    loads[11].wait()

    half_rows = heads * HEAD
    half_cols = wo.shape[1] // 2
    own_rows = pl.ds(pl.multiple_of(group * half_rows, half_rows), half_rows)
    other_rows = pl.ds(pl.multiple_of((1 - group) * half_rows, half_rows), half_rows)
    own_cols = pl.ds(pl.multiple_of(group * half_cols, half_cols), half_cols)
    other_cols = pl.ds(pl.multiple_of((1 - group) * half_cols, half_cols), half_cols)

    def project_block(j, carry):
        for b in range(2):
            mix_copy(2 * j + b).wait_recv()
        part = pl.ds(pl.multiple_of(2 * j * SEL, 2 * SEL), 2 * SEL)
        own, other = mixed_own[part, :], mixed_other[part, :]
        mine = dot(own, wo[own_rows, own_cols]) + dot(other, wo[other_rows, own_cols])
        rest = dot(own, wo[own_rows, other_cols]) + dot(other, wo[other_rows, other_cols])
        power = jnp.sum(mine * mine + rest * rest, axis=1, keepdims=True)
        scale = lax.rsqrt(power / wo.shape[1] + EPS)
        out_ref[part, :] = (mine * scale * gain_ref[:, own_cols]).astype(BF16)
        return carry

    lax.fori_loop(0, blocks // 2, project_block, 0)

    def end_mix(j, carry):
        mix_copy(j).wait_send()
        return carry

    lax.fori_loop(0, blocks, end_mix, 0)

    def end_sends(step, carry):
        pre_copy(me, spans - 1 - step).wait_send()
        kv_copy(me, spans - 1 - step).wait_send()
        return carry

    lax.fori_loop(0, spans - 1 - me, end_sends, 0)

    def end_asks(span, carry):
        ask_copy(me, span).wait_send()
        return carry

    lax.fori_loop(0, me, end_asks, 0)


def local(spans, tokens, chosen, *weights):
    w_query, w_ks, w_vs, w_kc, w_vc, ski, sko, svi, svo, w_gates, w_out, gain = weights
    rows, width = tokens.shape
    heads = w_query.shape[1] // HEAD
    blocks = rows // SEL
    cmp_rows = rows // CMP_STRIDE
    any_spec = pl.BlockSpec(memory_space=pl.ANY)
    vmem = pl.BlockSpec(memory_space=pltpu.VMEM)
    dma = pltpu.SemaphoreType.DMA
    return pl.pallas_call(
        functools.partial(kernel, spans),
        out_shape=jax.ShapeDtypeStruct((rows, w_out.shape[1] // 2), BF16),
        in_specs=[any_spec, vmem] + [any_spec] * 11 + [vmem],
        out_specs=vmem,
        scratch_shapes=[
            pltpu.VMEM(tokens.shape, BF16),
            pltpu.VMEM(w_query.shape, BF16),
            pltpu.VMEM((width, 2 * w_ks.shape[1]), BF16),
            pltpu.VMEM((width, 2 * w_kc.shape[1]), BF16),
            pltpu.VMEM(ski.shape[::-1], BF16),
            pltpu.VMEM(sko.shape, BF16),
            pltpu.VMEM(svi.shape[::-1], BF16),
            pltpu.VMEM(svo.shape, BF16),
            pltpu.VMEM(w_gates.shape[::-1], BF16),
            pltpu.VMEM(w_out.shape, BF16),
            pltpu.VMEM((rows, LANES), F32),
            pltpu.VMEM((rows, LANES), BF16),
            pltpu.VMEM((spans, CAP * SEL, LANES), BF16),
            pltpu.VMEM((spans, CAP * SEL, LANES), BF16),
            pltpu.VMEM((spans,) + chosen.shape, jnp.int32),
            pltpu.VMEM((spans * CAP, LANES), jnp.int32),
            pltpu.VMEM((spans, cmp_rows + 8, LANES), F32),
            pltpu.VMEM((spans * cmp_rows, LANES), BF16),
            pltpu.VMEM((blocks, heads * SEL, LANES), BF16),
            pltpu.VMEM((rows, 2 * heads), F32),
            pltpu.VMEM((blocks, rows), F32),
            pltpu.VMEM((spans, blocks, CAP * SEL), F32),
            pltpu.VMEM((blocks, heads * SEL, LANES), F32),
            pltpu.VMEM((blocks, heads * SEL, LANES), F32),
            pltpu.VMEM((blocks, heads * SEL, LANES), F32),
            pltpu.VMEM((rows, heads * HEAD), BF16),
            pltpu.VMEM((rows, heads * HEAD), BF16),
            dma((12,)),
            dma((spans,)),
            dma((spans,)),
            dma((spans,)),
            dma((spans,)),
            dma((spans,)),
            dma((spans,)),
            dma((blocks,)),
            dma((blocks,)),
        ],
        compiler_params=pltpu.CompilerParams(collective_id=0, has_side_effects=True),
    )(
        tokens,
        chosen,
        w_query,
        w_ks,
        w_vs,
        w_kc,
        w_vc,
        ski.T,
        sko,
        svi.T,
        svo,
        w_gates.T,
        w_out,
        gain.reshape(1, -1),
    )


def solution(mesh):
    in_specs = (
        P(("dp", "kv"), None),
        P(("dp", "kv"), "tp", None),
        P(None, "tp"),
    ) + (P(),) * 11
    return jax.shard_map(
        functools.partial(local, mesh.shape["kv"]),
        mesh=mesh,
        in_specs=in_specs,
        out_specs=P(("dp", "kv"), "tp"),
        check_vma=False,
    )
```

```python
import functools

import jax
import jax.numpy as jnp
from jax import lax
from jax.experimental import pallas as pl
from jax.experimental.pallas import tpu as pltpu
from jax.sharding import PartitionSpec as P

HEAD = 64
CMP_STRIDE = 16
CMP_LEN = 32
SEL = 64
CAP = 4
FAR = 3
LANES = 128
EPS = 1e-06
NEG = -1e30
MESH = pl.DeviceIdType.MESH
F32 = jnp.float32
BF16 = jnp.bfloat16


def dot(a, b):
    return jnp.dot(a, b, preferred_element_type=F32)


def dot_t(a, b):
    return lax.dot_general(a, b, (((1,), (1,)), ((), ())), preferred_element_type=F32)


def swap(x):
    return pltpu.roll(x, HEAD, 1)


def low_lanes(shape):
    return lax.broadcasted_iota(jnp.int32, shape, 1) < HEAD


def kernel(
    spans,
    tokens_h,
    chosen_ref,
    wq_h,
    wks_h,
    wvs_h,
    wkc_h,
    wvc_h,
    ski_h,
    sko_h,
    svi_h,
    svo_h,
    wg_h,
    wo_h,
    gain_ref,
    out_ref,
    tokens,
    wq,
    wsum,
    wcho,
    ski,
    sko,
    svi,
    svo,
    wg,
    wo,
    raw,
    kv_own,
    kv_all,
    packed,
    asks,
    slots,
    pre_all,
    sum_kv,
    q_s,
    gates,
    bias,
    far_bias,
    acc,
    m_s,
    l_s,
    sum_out,
    gate_s,
    mixed_own,
    mixed_other,
    in_sem,
    ask_send,
    ask_recv,
    kv_send,
    kv_recv,
    pre_send,
    pre_recv,
    mix_send,
    mix_recv,
):
    me = lax.axis_index("kv")
    group = lax.axis_index("tp")
    first = group == 0
    rows, _ = tokens.shape
    blocks = rows // SEL
    cmp_rows = rows // CMP_STRIDE
    heads = wq.shape[1] // HEAD
    q_rows = heads * SEL
    chunks, far_keys = far_bias.shape[0], far_bias.shape[2]
    per_chunk = far_keys // (CAP * SEL)

    loads = [
        pltpu.make_async_copy(src, dst, in_sem.at[i])
        for i, (src, dst) in enumerate(
            [
                (wkc_h, wcho.at[:, pl.ds(0, LANES)]),
                (wvc_h, wcho.at[:, pl.ds(LANES, LANES)]),
                (tokens_h, tokens),
                (wks_h, wsum.at[:, pl.ds(0, LANES)]),
                (wvs_h, wsum.at[:, pl.ds(LANES, LANES)]),
                (ski_h, ski),
                (svi_h, svi),
                (wq_h, wq),
                (wg_h, wg),
                (sko_h, sko),
                (svo_h, svo),
                (wo_h, wo),
            ]
        )
    ]
    for load in loads:
        load.start()

    barrier = pltpu.get_barrier_semaphore()

    def greet(step, carry):
        other = lax.rem(me + step, spans)
        pl.semaphore_signal(barrier, inc=1, device_id={"kv": other}, device_id_type=MESH)
        return carry

    lax.fori_loop(1, spans, greet, 0)
    pl.semaphore_signal(barrier, inc=1, device_id={"tp": 1 - group}, device_id_type=MESH)

    low = low_lanes((rows, LANES))

    def ask_copy(source, target):
        return pltpu.make_async_remote_copy(
            src_ref=chosen_ref,
            dst_ref=asks.at[source],
            send_sem=ask_send.at[target],
            recv_sem=ask_recv.at[source],
            device_id={"kv": target},
            device_id_type=MESH,
        )

    def kv_copy(source, target):
        return pltpu.make_async_remote_copy(
            src_ref=packed.at[target],
            dst_ref=kv_all.at[source],
            send_sem=kv_send.at[target],
            recv_sem=kv_recv.at[source],
            device_id={"kv": target},
            device_id_type=MESH,
        )

    pl.semaphore_wait(barrier, spans)

    def send_ask(span, carry):
        ask_copy(me, span).start()
        return carry

    lax.fori_loop(0, me, send_ask, 0)

    def block_of_slot(picks):
        lanes = -(-spans * blocks // LANES) * LANES
        ids = lax.broadcasted_iota(jnp.int32, (blocks, lanes), 1)
        hit = jnp.zeros((blocks, lanes), jnp.int32)
        for t in range(picks.shape[1]):
            hit = jnp.where(picks[:, t : t + 1] == ids, 1, hit)
        need = jnp.broadcast_to(jnp.max(hit, axis=0, keepdims=True), (8, lanes))
        lane = lax.broadcasted_iota(jnp.int32, (8, lanes), 1)
        rank = jnp.zeros((8, lanes), jnp.int32)
        for d in range(1, blocks):
            rank = rank + jnp.where(lane % blocks >= d, pltpu.roll(need, d, 1), 0)
        code = jnp.where((need > 0) & (rank < CAP), lane // blocks * CAP + rank, -1)[:1]
        place = lax.broadcasted_iota(jnp.int32, (slots.shape[0], lanes), 0)
        id_row = lax.broadcasted_iota(jnp.int32, (slots.shape[0], lanes), 1)
        found = jnp.where(code == place, id_row, -1)
        return jnp.broadcast_to(jnp.max(found, axis=1, keepdims=True), slots.shape)

    def pair(both):
        k2, v2 = both[:, :LANES], both[:, LANES:]
        k_side = jnp.where(first, k2, swap(k2))
        v_side = jnp.where(first, swap(v2), v2)
        return jnp.where(low, k_side, v_side)

    for load in loads[:3]:
        load.wait()
    kv_own[...] = pair(dot(tokens[...], wcho[...])).astype(BF16)

    for load in loads[3:5]:
        load.wait()
    raw[...] = pair(dot(tokens[...], wsum[...]))

    for load in loads[5:7]:
        load.wait()
    low_c = low_lanes((cmp_rows, LANES))
    key_tiles, value_tiles = [], []
    for a in range(CMP_STRIDE // 2):
        even = raw[pl.ds(2 * a, cmp_rows, stride=CMP_STRIDE), :]
        odd = raw[pl.ds(2 * a + 1, cmp_rows, stride=CMP_STRIDE), :]
        key_tiles.append(jnp.where(low_c, even, swap(odd)).astype(BF16))
        value_tiles.append(jnp.where(low_c, swap(even), odd).astype(BF16))
    half = CMP_STRIDE * HEAD
    joined_k = jnp.concatenate(key_tiles, axis=1)
    joined_v = jnp.concatenate(value_tiles, axis=1)
    head_sum = jnp.concatenate(
        [dot_t(joined_k, ski[:, pl.ds(0, half)]), dot_t(joined_v, svi[:, pl.ds(0, half)])], axis=1
    )
    tail_sum = jnp.concatenate(
        [dot_t(joined_k, ski[:, pl.ds(half, half)]), dot_t(joined_v, svi[:, pl.ds(half, half)])], axis=1
    )
    row_c = lax.broadcasted_iota(jnp.int32, (cmp_rows, LANES), 0)
    shifted = jnp.where(row_c < cmp_rows - 1, pltpu.roll(tail_sum, cmp_rows - 1, 0), 0.0)
    pre_all[me, pl.ds(0, cmp_rows), :] = head_sum + shifted
    pre_all[me, pl.ds(cmp_rows, 8), :] = tail_sum[:8]

    def clear(span, carry):
        pre_all[span] = jnp.zeros(pre_all.shape[1:], F32)
        return carry

    lax.fori_loop(me + 1, spans, clear, 0)

    def pre_copy(source, target):
        return pltpu.make_async_remote_copy(
            src_ref=pre_all.at[source],
            dst_ref=pre_all.at[source],
            send_sem=pre_send.at[target],
            recv_sem=pre_recv.at[source],
            device_id={"kv": target},
            device_id_type=MESH,
        )

    def send_pre(step, carry):
        pre_copy(me, spans - 1 - step).start()
        return carry

    lax.fori_loop(0, spans - 1 - me, send_pre, 0)

    def serve(step, carry):
        target = spans - 1 - step
        ask_copy(target, me).wait_recv()
        slots[...] = block_of_slot(asks[target][:, 0, :])
        key_lane = lax.broadcasted_iota(jnp.int32, (SEL, rows), 1)
        key_row = lax.broadcasted_iota(jnp.int32, (SEL, rows), 0)
        ours = slots[pl.ds(me * CAP, CAP), :]
        pieces = []
        for k in range(CAP):
            start = (ours[k : k + 1, :1] - me * blocks) * SEL
            pieces.append(jnp.where(key_lane == start + key_row, 1.0, 0.0).astype(BF16))
        packed[target] = dot(jnp.concatenate(pieces, axis=0), kv_own[...]).astype(BF16)
        kv_copy(me, target).start()
        return carry

    lax.fori_loop(0, spans - 1 - me, serve, 0)

    for load in loads[7:9]:
        load.wait()
    scaled = dot(tokens[...], wq[...]).astype(BF16).astype(F32) * (HEAD**-0.5)
    for a in range(heads // 2):
        tile = scaled[:, a * LANES : (a + 1) * LANES]
        even = jnp.where(low, tile, 0.0).astype(BF16)
        odd = jnp.where(low, swap(tile), 0.0).astype(BF16)
        q_s[:, pl.ds(2 * a * SEL, SEL), :] = even.reshape(blocks, SEL, LANES)
        q_s[:, pl.ds((2 * a + 1) * SEL, SEL), :] = odd.reshape(blocks, SEL, LANES)
    gate_all = jax.nn.sigmoid(dot_t(tokens[...], wg[...]))
    width = 2 * heads
    gates[...] = jnp.where(first, gate_all[:, :width], gate_all[:, width : 2 * width])

    picks = chosen_ref[:, 0, :]

    def bias_of(ids):
        hit = jnp.zeros((blocks, ids.shape[1]), F32)
        for t in range(picks.shape[1]):
            hit = jnp.where(picks[:, t : t + 1] == ids, 1.0, hit)
        return jnp.where(hit > 0.0, 0.0, NEG)

    def lane_sum(p):
        total = p[:, :LANES]
        for c in range(1, p.shape[1] // LANES):
            total = total + p[:, c * LANES : (c + 1) * LANES]
        return total

    bias[...] = bias_of(me * blocks + lax.broadcasted_iota(jnp.int32, (blocks, rows), 1) // SEL)
    slots[...] = block_of_slot(picks)
    low_b = low_lanes((blocks, LANES))
    for c in range(chunks):
        tiles = []
        for span in range(c * per_chunk, (c + 1) * per_chunk):
            ids = slots[pl.ds(span * CAP, CAP), :]
            ids = jnp.where(span < me, ids, -1)
            for a in range(CAP // 2):
                tiles.append(jnp.where(low_b, ids[2 * a : 2 * a + 1], ids[2 * a + 1 : 2 * a + 2]))
        far_bias[c] = bias_of(jnp.concatenate(tiles, axis=1))

    def clear_far(span, carry):
        kv_all[span] = jnp.zeros(kv_all.shape[1:], BF16)
        return carry

    lax.fori_loop(me, chunks * per_chunk, clear_far, 0)

    lane_q = lax.broadcasted_iota(jnp.int32, (q_rows, LANES), 1)
    row_q = lax.broadcasted_iota(jnp.int32, (q_rows, LANES), 0) % SEL
    for jj in range(blocks // 2):
        keys = kv_own[: (jj + 1) * 2 * SEL]
        for odd in range(2):
            j = 2 * jj + odd
            scores = dot_t(q_s[j], keys) + bias[j : j + 1, : keys.shape[0]]
            tail = jnp.where(lane_q <= row_q + odd * SEL, scores[:, -LANES:], NEG)
            if jj > 0:
                tail = jnp.concatenate([scores[:, :-LANES], tail], axis=1)
            peak = jnp.max(tail, axis=1, keepdims=True)
            p = jnp.exp(tail - peak)
            m_s[j] = jnp.broadcast_to(peak, (q_rows, LANES))
            l_s[j] = lane_sum(p)
            acc[j] = dot(p.astype(BF16), keys)

    def await_pre(span, carry):
        pre_copy(span, me).wait_recv()
        return carry

    lax.fori_loop(0, me, await_pre, 0)
    for load in loads[9:11]:
        load.wait()
    parts = []
    for span in range(spans):
        part = pre_all[span, pl.ds(0, cmp_rows), :]
        if span + 1 < spans:
            part = part + jnp.where(
                row_c == cmp_rows - 1, pre_all[span + 1, pl.ds(cmp_rows, 1), :], 0.0
            )
        parts.append(part)
    hidden = jax.nn.gelu(jnp.concatenate(parts, axis=0)).astype(BF16)
    sum_kv[...] = jnp.concatenate(
        [dot(hidden[:, :HEAD], sko[...]), dot(hidden[:, HEAD:], svo[...])], axis=1
    ).astype(BF16)

    def summarized(j):
        table = sum_kv[...]
        scores = dot_t(q_s[j], table)
        ends = lax.broadcasted_iota(jnp.int32, scores.shape, 1) * CMP_STRIDE + CMP_LEN - 1
        time = me * rows + j * SEL + lax.broadcasted_iota(jnp.int32, scores.shape, 0) % SEL
        visible = ends <= time
        scores = jnp.where(visible, scores, NEG)
        peak = jnp.max(scores, axis=1, keepdims=True)
        p = jnp.where(visible, jnp.exp(scores - peak), 0.0)
        weight = jnp.sum(p, axis=1, keepdims=True)
        gate = gates[pl.ds(pl.multiple_of(j * SEL, SEL), SEL), :]
        near = jnp.concatenate([gate[:, 2 * h : 2 * h + 1] for h in range(heads)], axis=0)
        far = jnp.concatenate([gate[:, 2 * h + 1 : 2 * h + 2] for h in range(heads)], axis=0)
        factor = near / jnp.where(weight > 0.0, weight, 1.0)
        return dot(p.astype(BF16), table) * factor, jnp.broadcast_to(far, (q_rows, LANES))

    def summary_pair(jj, carry):
        both = (2 * jj, 2 * jj + 1)
        for j, (total, far) in zip(both, [summarized(j) for j in both]):
            sum_out[j] = total
            gate_s[j] = far
        return carry

    lax.fori_loop(0, blocks // 2, summary_pair, 0)

    def merged(j, chunk):
        keys = kv_all[pl.ds(chunk * per_chunk, per_chunk)].reshape(far_keys, LANES)
        scores = dot_t(q_s[j], keys) + far_bias[chunk, pl.ds(j, 1), :]
        old = m_s[j]
        peak = jnp.maximum(old, jnp.max(scores, axis=1, keepdims=True))
        p = jnp.concatenate(
            [jnp.exp(scores[:, c : c + LANES] - peak) for c in range(0, far_keys, LANES)], axis=1
        )
        fix = jnp.exp(old - peak)
        return peak, l_s[j] * fix + lane_sum(p), acc[j] * fix + dot(p.astype(BF16), keys)

    def await_far(span, carry):
        kv_copy(span, me).wait_recv()
        return carry

    def chunk_step(step, carry):
        chunk = chunks - 1 - step
        lax.fori_loop(
            chunk * per_chunk, jnp.minimum((chunk + 1) * per_chunk, me), await_far, 0
        )

        def update(j, inner):
            peak, weight, total = merged(j, chunk)
            m_s[j] = peak
            l_s[j] = weight
            acc[j] = total
            return inner

        return lax.fori_loop(0, blocks, update, carry)

    if chunks > 1:
        lax.fori_loop(0, chunks - 1, chunk_step, 0)

    lax.fori_loop(0, jnp.minimum(per_chunk, me), await_far, 0)
    low_q = low_lanes((SEL, LANES))

    def mix_copy(j):
        part = pl.ds(pl.multiple_of(j * SEL, SEL), SEL)
        return pltpu.make_async_remote_copy(
            src_ref=mixed_own.at[part, :],
            dst_ref=mixed_other.at[part, :],
            send_sem=mix_send.at[j],
            recv_sem=mix_recv.at[j],
            device_id={"tp": 1 - group},
            device_id_type=MESH,
        )

    def finished(j):
        _, weight, total = merged(j, 0)
        mixed = sum_out[j] + total * (gate_s[j] / jnp.sum(weight, axis=1, keepdims=True))
        part = pl.ds(pl.multiple_of(j * SEL, SEL), SEL)
        tiles = []
        for a in range(heads // 2):
            even = mixed[2 * a * SEL : (2 * a + 1) * SEL]
            odd = mixed[(2 * a + 1) * SEL : (2 * a + 2) * SEL]
            tiles.append(jnp.where(low_q, swap(even), odd))
        return part, jnp.concatenate(tiles, axis=1).astype(BF16)

    def finish_pair(jj, carry):
        both = (2 * jj, 2 * jj + 1)
        for part, mixed in [finished(j) for j in both]:
            mixed_own[part, :] = mixed
        for j in both:
            mix_copy(j).start()
        return carry

    lax.fori_loop(0, blocks // 2, finish_pair, 0)
    loads[11].wait()

    half_rows = heads * HEAD
    half_cols = wo.shape[1] // 2
    own_rows = pl.ds(pl.multiple_of(group * half_rows, half_rows), half_rows)
    other_rows = pl.ds(pl.multiple_of((1 - group) * half_rows, half_rows), half_rows)
    own_cols = pl.ds(pl.multiple_of(group * half_cols, half_cols), half_cols)
    other_cols = pl.ds(pl.multiple_of((1 - group) * half_cols, half_cols), half_cols)

    def project_block(j, carry):
        for b in range(2):
            mix_copy(2 * j + b).wait_recv()
        part = pl.ds(pl.multiple_of(2 * j * SEL, 2 * SEL), 2 * SEL)
        own, other = mixed_own[part, :], mixed_other[part, :]
        mine = dot(own, wo[own_rows, own_cols]) + dot(other, wo[other_rows, own_cols])
        rest = dot(own, wo[own_rows, other_cols]) + dot(other, wo[other_rows, other_cols])
        power = jnp.sum(mine * mine + rest * rest, axis=1, keepdims=True)
        scale = lax.rsqrt(power / wo.shape[1] + EPS)
        out_ref[part, :] = (mine * scale * gain_ref[:, own_cols]).astype(BF16)
        return carry

    lax.fori_loop(0, blocks // 2, project_block, 0)

    def end_mix(j, carry):
        mix_copy(j).wait_send()
        return carry

    lax.fori_loop(0, blocks, end_mix, 0)

    def end_sends(step, carry):
        pre_copy(me, spans - 1 - step).wait_send()
        kv_copy(me, spans - 1 - step).wait_send()
        return carry

    lax.fori_loop(0, spans - 1 - me, end_sends, 0)

    def end_asks(span, carry):
        ask_copy(me, span).wait_send()
        return carry

    lax.fori_loop(0, me, end_asks, 0)


def local(spans, tokens, chosen, *weights):
    w_query, w_ks, w_vs, w_kc, w_vc, ski, sko, svi, svo, w_gates, w_out, gain = weights
    rows, width = tokens.shape
    heads = w_query.shape[1] // HEAD
    blocks = rows // SEL
    cmp_rows = rows // CMP_STRIDE
    per_chunk = min(FAR, spans - 1)
    chunks = -(-(spans - 1) // per_chunk)
    any_spec = pl.BlockSpec(memory_space=pl.ANY)
    vmem = pl.BlockSpec(memory_space=pltpu.VMEM)
    dma = pltpu.SemaphoreType.DMA
    return pl.pallas_call(
        functools.partial(kernel, spans),
        out_shape=jax.ShapeDtypeStruct((rows, w_out.shape[1] // 2), BF16),
        in_specs=[any_spec, vmem] + [any_spec] * 11 + [vmem],
        out_specs=vmem,
        scratch_shapes=[
            pltpu.VMEM(tokens.shape, BF16),
            pltpu.VMEM(w_query.shape, BF16),
            pltpu.VMEM((width, 2 * w_ks.shape[1]), BF16),
            pltpu.VMEM((width, 2 * w_kc.shape[1]), BF16),
            pltpu.VMEM(ski.shape[::-1], BF16),
            pltpu.VMEM(sko.shape, BF16),
            pltpu.VMEM(svi.shape[::-1], BF16),
            pltpu.VMEM(svo.shape, BF16),
            pltpu.VMEM(w_gates.shape[::-1], BF16),
            pltpu.VMEM(w_out.shape, BF16),
            pltpu.VMEM((rows, LANES), F32),
            pltpu.VMEM((rows, LANES), BF16),
            pltpu.VMEM((chunks * per_chunk, CAP * SEL, LANES), BF16),
            pltpu.VMEM((spans, CAP * SEL, LANES), BF16),
            pltpu.VMEM((spans,) + chosen.shape, jnp.int32),
            pltpu.VMEM((max(spans, chunks * per_chunk) * CAP, LANES), jnp.int32),
            pltpu.VMEM((spans, cmp_rows + 8, LANES), F32),
            pltpu.VMEM((spans * cmp_rows, LANES), BF16),
            pltpu.VMEM((blocks, heads * SEL, LANES), BF16),
            pltpu.VMEM((rows, 2 * heads), F32),
            pltpu.VMEM((blocks, rows), F32),
            pltpu.VMEM((chunks, blocks, per_chunk * CAP * SEL), F32),
            pltpu.VMEM((blocks, heads * SEL, LANES), F32),
            pltpu.VMEM((blocks, heads * SEL, LANES), F32),
            pltpu.VMEM((blocks, heads * SEL, LANES), F32),
            pltpu.VMEM((blocks, heads * SEL, LANES), F32),
            pltpu.VMEM((blocks, heads * SEL, LANES), F32),
            pltpu.VMEM((rows, heads * HEAD), BF16),
            pltpu.VMEM((rows, heads * HEAD), BF16),
            dma((12,)),
            dma((spans,)),
            dma((spans,)),
            dma((spans,)),
            dma((spans,)),
            dma((spans,)),
            dma((spans,)),
            dma((blocks,)),
            dma((blocks,)),
        ],
        compiler_params=pltpu.CompilerParams(collective_id=0, has_side_effects=True),
    )(
        tokens,
        chosen,
        w_query,
        w_ks,
        w_vs,
        w_kc,
        w_vc,
        ski.T,
        sko,
        svi.T,
        svo,
        w_gates.T,
        w_out,
        gain.reshape(1, -1),
    )


def solution(mesh):
    in_specs = (
        P(("dp", "kv"), None),
        P(("dp", "kv"), "tp", None),
        P(None, "tp"),
    ) + (P(),) * 11
    return jax.shard_map(
        functools.partial(local, mesh.shape["kv"]),
        mesh=mesh,
        in_specs=in_specs,
        out_specs=P(("dp", "kv"), "tp"),
        check_vma=False,
    )
```

```python
import functools

import jax
import jax.numpy as jnp
from jax import lax
from jax.experimental import pallas as pl
from jax.experimental.pallas import tpu as pltpu
from jax.sharding import PartitionSpec as P

HEAD = 64
CMP_STRIDE = 16
CMP_LEN = 32
SEL = 64
CAP = 4
FAR = 3
WIDE = 4
LANES = 128
EPS = 1e-06
NEG = -1e30
MESH = pl.DeviceIdType.MESH
F32 = jnp.float32
BF16 = jnp.bfloat16


def dot(a, b):
    return jnp.dot(a, b, preferred_element_type=F32)


def dot_t(a, b):
    return lax.dot_general(a, b, (((1,), (1,)), ((), ())), preferred_element_type=F32)


def swap(x):
    return pltpu.roll(x, HEAD, 1)


def low_lanes(shape):
    return lax.broadcasted_iota(jnp.int32, shape, 1) < HEAD


def kernel(
    spans,
    tokens_h,
    chosen_ref,
    wq_h,
    wks_h,
    wvs_h,
    wkc_h,
    wvc_h,
    ski_h,
    sko_h,
    svi_h,
    svo_h,
    wg_h,
    wo_h,
    gain_ref,
    out_ref,
    tokens,
    wq,
    wsum,
    wcho,
    ski,
    sko,
    svi,
    svo,
    wg,
    wo,
    raw,
    kv_own,
    kv_all,
    packed,
    asks,
    slots,
    pre_all,
    sum_kv,
    q_s,
    gates,
    bias,
    far_bias,
    acc,
    m_s,
    l_s,
    sum_out,
    gate_s,
    mixed_own,
    mixed_other,
    in_sem,
    ask_send,
    ask_recv,
    kv_send,
    kv_recv,
    pre_send,
    pre_recv,
    mix_send,
    mix_recv,
):
    me = lax.axis_index("kv")
    group = lax.axis_index("tp")
    first = group == 0
    rows, _ = tokens.shape
    blocks = rows // SEL
    cmp_rows = rows // CMP_STRIDE
    heads = wq.shape[1] // HEAD
    q_rows = heads * SEL
    chunks, far_keys = far_bias.shape[0], far_bias.shape[2]
    per_chunk = far_keys // (CAP * SEL)

    loads = [
        pltpu.make_async_copy(src, dst, in_sem.at[i])
        for i, (src, dst) in enumerate(
            [
                (wkc_h, wcho.at[:, pl.ds(0, LANES)]),
                (wvc_h, wcho.at[:, pl.ds(LANES, LANES)]),
                (tokens_h, tokens),
                (wks_h, wsum.at[:, pl.ds(0, LANES)]),
                (wvs_h, wsum.at[:, pl.ds(LANES, LANES)]),
                (ski_h, ski),
                (svi_h, svi),
                (wq_h, wq),
                (wg_h, wg),
                (sko_h, sko),
                (svo_h, svo),
                (wo_h, wo),
            ]
        )
    ]
    for load in loads:
        load.start()

    barrier = pltpu.get_barrier_semaphore()

    def greet(step, carry):
        other = lax.rem(me + step, spans)
        pl.semaphore_signal(barrier, inc=1, device_id={"kv": other}, device_id_type=MESH)
        return carry

    lax.fori_loop(1, spans, greet, 0)
    pl.semaphore_signal(barrier, inc=1, device_id={"tp": 1 - group}, device_id_type=MESH)

    low = low_lanes((rows, LANES))

    def ask_copy(source, target):
        return pltpu.make_async_remote_copy(
            src_ref=chosen_ref,
            dst_ref=asks.at[source],
            send_sem=ask_send.at[target],
            recv_sem=ask_recv.at[source],
            device_id={"kv": target},
            device_id_type=MESH,
        )

    def kv_copy(source, target):
        return pltpu.make_async_remote_copy(
            src_ref=packed.at[target],
            dst_ref=kv_all.at[source],
            send_sem=kv_send.at[target],
            recv_sem=kv_recv.at[source],
            device_id={"kv": target},
            device_id_type=MESH,
        )

    def send_ask(span, carry):
        ask_copy(me, span).start()
        return carry

    def enter():
        pl.semaphore_wait(barrier, spans)
        lax.fori_loop(0, me, send_ask, 0)

    pl.when(me >= spans // 2)(enter)

    def block_of_slot(picks):
        lanes = -(-spans * blocks // LANES) * LANES
        ids = lax.broadcasted_iota(jnp.int32, (blocks, lanes), 1)
        hit = jnp.zeros((blocks, lanes), jnp.int32)
        for t in range(picks.shape[1]):
            hit = jnp.where(picks[:, t : t + 1] == ids, 1, hit)
        need = jnp.broadcast_to(jnp.max(hit, axis=0, keepdims=True), (8, lanes))
        lane = lax.broadcasted_iota(jnp.int32, (8, lanes), 1)
        rank = jnp.zeros((8, lanes), jnp.int32)
        for d in range(1, blocks):
            rank = rank + jnp.where(lane % blocks >= d, pltpu.roll(need, d, 1), 0)
        code = jnp.where((need > 0) & (rank < CAP), lane // blocks * CAP + rank, -1)[:1]
        place = lax.broadcasted_iota(jnp.int32, (slots.shape[0], lanes), 0)
        id_row = lax.broadcasted_iota(jnp.int32, (slots.shape[0], lanes), 1)
        found = jnp.where(code == place, id_row, -1)
        return jnp.broadcast_to(jnp.max(found, axis=1, keepdims=True), slots.shape)

    def pair(both):
        k2, v2 = both[:, :LANES], both[:, LANES:]
        k_side = jnp.where(first, k2, swap(k2))
        v_side = jnp.where(first, swap(v2), v2)
        return jnp.where(low, k_side, v_side)

    for load in loads[:3]:
        load.wait()
    kv_own[...] = pair(dot(tokens[...], wcho[...])).astype(BF16)

    for load in loads[3:5]:
        load.wait()
    raw[...] = pair(dot(tokens[...], wsum[...]))

    for load in loads[5:7]:
        load.wait()
    low_c = low_lanes((cmp_rows, LANES))
    key_tiles, value_tiles = [], []
    for a in range(CMP_STRIDE // 2):
        even = raw[pl.ds(2 * a, cmp_rows, stride=CMP_STRIDE), :]
        odd = raw[pl.ds(2 * a + 1, cmp_rows, stride=CMP_STRIDE), :]
        key_tiles.append(jnp.where(low_c, even, swap(odd)).astype(BF16))
        value_tiles.append(jnp.where(low_c, swap(even), odd).astype(BF16))
    half = CMP_STRIDE * HEAD
    joined_k = jnp.concatenate(key_tiles, axis=1)
    joined_v = jnp.concatenate(value_tiles, axis=1)
    head_sum = jnp.concatenate(
        [dot_t(joined_k, ski[:, pl.ds(0, half)]), dot_t(joined_v, svi[:, pl.ds(0, half)])], axis=1
    )
    tail_sum = jnp.concatenate(
        [dot_t(joined_k, ski[:, pl.ds(half, half)]), dot_t(joined_v, svi[:, pl.ds(half, half)])], axis=1
    )
    row_c = lax.broadcasted_iota(jnp.int32, (cmp_rows, LANES), 0)
    shifted = jnp.where(row_c < cmp_rows - 1, pltpu.roll(tail_sum, cmp_rows - 1, 0), 0.0)
    pre_all[me, pl.ds(0, cmp_rows), :] = head_sum + shifted
    pre_all[me, pl.ds(cmp_rows, 8), :] = tail_sum[:8]

    def clear(span, carry):
        pre_all[span] = jnp.zeros(pre_all.shape[1:], F32)
        return carry

    lax.fori_loop(me + 1, spans, clear, 0)

    def pre_copy(source, target):
        return pltpu.make_async_remote_copy(
            src_ref=pre_all.at[source],
            dst_ref=pre_all.at[source],
            send_sem=pre_send.at[target],
            recv_sem=pre_recv.at[source],
            device_id={"kv": target},
            device_id_type=MESH,
        )

    pl.when(me < spans // 2)(enter)

    def send_pre(step, carry):
        pre_copy(me, spans - 1 - step).start()
        return carry

    lax.fori_loop(0, spans - 1 - me, send_pre, 0)


    for load in loads[7:9]:
        load.wait()
    scaled = dot(tokens[...], wq[...]).astype(BF16).astype(F32) * (HEAD**-0.5)
    for a in range(heads // 2):
        tile = scaled[:, a * LANES : (a + 1) * LANES]
        even = jnp.where(low, tile, 0.0).astype(BF16)
        odd = jnp.where(low, swap(tile), 0.0).astype(BF16)
        q_s[:, pl.ds(2 * a * SEL, SEL), :] = even.reshape(blocks, SEL, LANES)
        q_s[:, pl.ds((2 * a + 1) * SEL, SEL), :] = odd.reshape(blocks, SEL, LANES)
    gate_all = jax.nn.sigmoid(dot_t(tokens[...], wg[...]))
    width = 2 * heads
    gates[...] = jnp.where(first, gate_all[:, :width], gate_all[:, width : 2 * width])

    picks = chosen_ref[:, 0, :]

    def bias_of(ids):
        hit = jnp.zeros((blocks, ids.shape[1]), F32)
        for t in range(picks.shape[1]):
            hit = jnp.where(picks[:, t : t + 1] == ids, 1.0, hit)
        return jnp.where(hit > 0.0, 0.0, NEG)

    def lane_sum(p):
        total = p[:, :LANES]
        for c in range(1, p.shape[1] // LANES):
            total = total + p[:, c * LANES : (c + 1) * LANES]
        return total

    def own_attention():
        bias[...] = bias_of(me * blocks + lax.broadcasted_iota(jnp.int32, (blocks, rows), 1) // SEL)
        lane_q = lax.broadcasted_iota(jnp.int32, (q_rows, LANES), 1)
        row_q = lax.broadcasted_iota(jnp.int32, (q_rows, LANES), 0) % SEL
        for jj in range(blocks // 2):
            keys = kv_own[: (jj + 1) * 2 * SEL]
            for odd in range(2):
                j = 2 * jj + odd
                scores = dot_t(q_s[j], keys) + bias[j : j + 1, : keys.shape[0]]
                tail = jnp.where(lane_q <= row_q + odd * SEL, scores[:, -LANES:], NEG)
                if jj > 0:
                    tail = jnp.concatenate([scores[:, :-LANES], tail], axis=1)
                peak = jnp.max(tail, axis=1, keepdims=True)
                p = jnp.exp(tail - peak)
                m_s[j] = jnp.broadcast_to(peak, (q_rows, LANES))
                l_s[j] = lane_sum(p)
                acc[j] = dot(p.astype(BF16), keys)

    pl.when(me == 0)(own_attention)

    def serve(step, carry):
        target = spans - 1 - step
        ask_copy(target, me).wait_recv()
        slots[...] = block_of_slot(asks[target][:, 0, :])
        key_lane = lax.broadcasted_iota(jnp.int32, (SEL, rows), 1)
        key_row = lax.broadcasted_iota(jnp.int32, (SEL, rows), 0)
        ours = slots[pl.ds(me * CAP, CAP), :]
        pieces = []
        for k in range(CAP):
            start = (ours[k : k + 1, :1] - me * blocks) * SEL
            pieces.append(jnp.where(key_lane == start + key_row, 1.0, 0.0).astype(BF16))
        packed[target] = dot(jnp.concatenate(pieces, axis=0), kv_own[...]).astype(BF16)
        kv_copy(me, target).start()
        return carry

    lax.fori_loop(0, spans - 1 - me, serve, 0)

    pl.when(me > 0)(own_attention)

    slots[...] = block_of_slot(picks)
    low_b = low_lanes((blocks, LANES))
    for c in range(chunks):
        tiles = []
        for span in range(c * per_chunk, (c + 1) * per_chunk):
            ids = slots[pl.ds(span * CAP, CAP), :]
            ids = jnp.where(span < me, ids, -1)
            for a in range(CAP // 2):
                tiles.append(jnp.where(low_b, ids[2 * a : 2 * a + 1], ids[2 * a + 1 : 2 * a + 2]))
        far_bias[c] = bias_of(jnp.concatenate(tiles, axis=1))

    def clear_far(span, carry):
        kv_all[span] = jnp.zeros(kv_all.shape[1:], BF16)
        return carry

    lax.fori_loop(me, chunks * per_chunk, clear_far, 0)

    def await_pre(span, carry):
        pre_copy(span, me).wait_recv()
        return carry

    lax.fori_loop(0, me, await_pre, 0)
    for load in loads[9:11]:
        load.wait()
    parts = []
    for span in range(spans):
        part = pre_all[span, pl.ds(0, cmp_rows), :]
        if span + 1 < spans:
            part = part + jnp.where(
                row_c == cmp_rows - 1, pre_all[span + 1, pl.ds(cmp_rows, 1), :], 0.0
            )
        parts.append(part)
    hidden = jax.nn.gelu(jnp.concatenate(parts, axis=0)).astype(BF16)
    sum_kv[...] = jnp.concatenate(
        [dot(hidden[:, :HEAD], sko[...]), dot(hidden[:, HEAD:], svo[...])], axis=1
    ).astype(BF16)

    def summarized(j):
        table = sum_kv[...]
        scores = dot_t(q_s[j], table)
        ends = lax.broadcasted_iota(jnp.int32, scores.shape, 1) * CMP_STRIDE + CMP_LEN - 1
        time = me * rows + j * SEL + lax.broadcasted_iota(jnp.int32, scores.shape, 0) % SEL
        visible = ends <= time
        scores = jnp.where(visible, scores, NEG)
        peak = jnp.max(scores, axis=1, keepdims=True)
        p = jnp.where(visible, jnp.exp(scores - peak), 0.0)
        weight = jnp.sum(p, axis=1, keepdims=True)
        gate = gates[j * SEL : (j + 1) * SEL, :]
        near = jnp.concatenate([gate[:, 2 * h : 2 * h + 1] for h in range(heads)], axis=0)
        far = jnp.concatenate([gate[:, 2 * h + 1 : 2 * h + 2] for h in range(heads)], axis=0)
        factor = near / jnp.where(weight > 0.0, weight, 1.0)
        return dot(p.astype(BF16), table) * factor, jnp.broadcast_to(far, (q_rows, LANES))

    for start in range(0, blocks, WIDE):
        some = range(start, start + WIDE)
        for j, (total, far) in zip(some, [summarized(j) for j in some]):
            sum_out[j] = total
            gate_s[j] = far

    def merged(j, chunk):
        keys = kv_all[pl.ds(chunk * per_chunk, per_chunk)].reshape(far_keys, LANES)
        scores = dot_t(q_s[j], keys) + far_bias[chunk, pl.ds(j, 1), :]
        old = m_s[j]
        peak = jnp.maximum(old, jnp.max(scores, axis=1, keepdims=True))
        p = jnp.concatenate(
            [jnp.exp(scores[:, c : c + LANES] - peak) for c in range(0, far_keys, LANES)], axis=1
        )
        fix = jnp.exp(old - peak)
        return peak, l_s[j] * fix + lane_sum(p), acc[j] * fix + dot(p.astype(BF16), keys)

    def await_far(span, carry):
        kv_copy(span, me).wait_recv()
        return carry

    def chunk_step(step, carry):
        chunk = chunks - 1 - step
        lax.fori_loop(
            chunk * per_chunk, jnp.minimum((chunk + 1) * per_chunk, me), await_far, 0
        )

        def update(j, inner):
            peak, weight, total = merged(j, chunk)
            m_s[j] = peak
            l_s[j] = weight
            acc[j] = total
            return inner

        return lax.fori_loop(0, blocks, update, carry)

    if chunks > 1:
        lax.fori_loop(0, chunks - 1, chunk_step, 0)

    lax.fori_loop(0, jnp.minimum(per_chunk, me), await_far, 0)
    low_q = low_lanes((SEL, LANES))

    def mix_copy(j):
        part = pl.ds(pl.multiple_of(j * SEL, SEL), SEL)
        return pltpu.make_async_remote_copy(
            src_ref=mixed_own.at[part, :],
            dst_ref=mixed_other.at[part, :],
            send_sem=mix_send.at[j],
            recv_sem=mix_recv.at[j],
            device_id={"tp": 1 - group},
            device_id_type=MESH,
        )

    def finished(j, far):
        _, weight, total = merged(j, 0) if far else (None, l_s[j], acc[j])
        mixed = sum_out[j] + total * (gate_s[j] / jnp.sum(weight, axis=1, keepdims=True))
        tiles = []
        for a in range(heads // 2):
            even = mixed[2 * a * SEL : (2 * a + 1) * SEL]
            odd = mixed[(2 * a + 1) * SEL : (2 * a + 2) * SEL]
            tiles.append(jnp.where(low_q, swap(even), odd))
        return jnp.concatenate(tiles, axis=1).astype(BF16)

    def finish_all(far):
        for start in range(0, blocks, WIDE):
            some = range(start, start + WIDE)
            for j, mixed in zip(some, [finished(j, far) for j in some]):
                mixed_own[j * SEL : (j + 1) * SEL, :] = mixed
            for j in some:
                mix_copy(j).start()

    pl.when(me == 0)(functools.partial(finish_all, False))
    pl.when(me > 0)(functools.partial(finish_all, True))
    loads[11].wait()

    half_rows = heads * HEAD
    half_cols = wo.shape[1] // 2
    own_rows = pl.ds(pl.multiple_of(group * half_rows, half_rows), half_rows)
    other_rows = pl.ds(pl.multiple_of((1 - group) * half_rows, half_rows), half_rows)
    own_cols = pl.ds(pl.multiple_of(group * half_cols, half_cols), half_cols)
    other_cols = pl.ds(pl.multiple_of((1 - group) * half_cols, half_cols), half_cols)

    gain = gain_ref[:, own_cols]
    for start in range(0, blocks, WIDE):
        for j in range(start, start + WIDE):
            mix_copy(j).wait_recv()
        part = pl.ds(start * SEL, WIDE * SEL)
        own, other = mixed_own[part, :], mixed_other[part, :]
        mine = dot(own, wo[own_rows, own_cols]) + dot(other, wo[other_rows, own_cols])
        rest = dot(own, wo[own_rows, other_cols]) + dot(other, wo[other_rows, other_cols])
        power = jnp.sum(mine * mine + rest * rest, axis=1, keepdims=True)
        out_ref[part, :] = (mine * lax.rsqrt(power / wo.shape[1] + EPS) * gain).astype(BF16)

    def end_mix(j, carry):
        mix_copy(j).wait_send()
        return carry

    lax.fori_loop(0, blocks, end_mix, 0)

    def end_sends(step, carry):
        pre_copy(me, spans - 1 - step).wait_send()
        kv_copy(me, spans - 1 - step).wait_send()
        return carry

    lax.fori_loop(0, spans - 1 - me, end_sends, 0)

    def end_asks(span, carry):
        ask_copy(me, span).wait_send()
        return carry

    lax.fori_loop(0, me, end_asks, 0)


def local(spans, tokens, chosen, *weights):
    w_query, w_ks, w_vs, w_kc, w_vc, ski, sko, svi, svo, w_gates, w_out, gain = weights
    rows, width = tokens.shape
    heads = w_query.shape[1] // HEAD
    blocks = rows // SEL
    cmp_rows = rows // CMP_STRIDE
    per_chunk = min(FAR, spans - 1)
    chunks = -(-(spans - 1) // per_chunk)
    any_spec = pl.BlockSpec(memory_space=pl.ANY)
    vmem = pl.BlockSpec(memory_space=pltpu.VMEM)
    dma = pltpu.SemaphoreType.DMA
    return pl.pallas_call(
        functools.partial(kernel, spans),
        out_shape=jax.ShapeDtypeStruct((rows, w_out.shape[1] // 2), BF16),
        in_specs=[any_spec, vmem] + [any_spec] * 11 + [vmem],
        out_specs=vmem,
        scratch_shapes=[
            pltpu.VMEM(tokens.shape, BF16),
            pltpu.VMEM(w_query.shape, BF16),
            pltpu.VMEM((width, 2 * w_ks.shape[1]), BF16),
            pltpu.VMEM((width, 2 * w_kc.shape[1]), BF16),
            pltpu.VMEM(ski.shape[::-1], BF16),
            pltpu.VMEM(sko.shape, BF16),
            pltpu.VMEM(svi.shape[::-1], BF16),
            pltpu.VMEM(svo.shape, BF16),
            pltpu.VMEM(w_gates.shape[::-1], BF16),
            pltpu.VMEM(w_out.shape, BF16),
            pltpu.VMEM((rows, LANES), F32),
            pltpu.VMEM((rows, LANES), BF16),
            pltpu.VMEM((chunks * per_chunk, CAP * SEL, LANES), BF16),
            pltpu.VMEM((spans, CAP * SEL, LANES), BF16),
            pltpu.VMEM((spans,) + chosen.shape, jnp.int32),
            pltpu.VMEM((max(spans, chunks * per_chunk) * CAP, LANES), jnp.int32),
            pltpu.VMEM((spans, cmp_rows + 8, LANES), F32),
            pltpu.VMEM((spans * cmp_rows, LANES), BF16),
            pltpu.VMEM((blocks, heads * SEL, LANES), BF16),
            pltpu.VMEM((rows, 2 * heads), F32),
            pltpu.VMEM((blocks, rows), F32),
            pltpu.VMEM((chunks, blocks, per_chunk * CAP * SEL), F32),
            pltpu.VMEM((blocks, heads * SEL, LANES), F32),
            pltpu.VMEM((blocks, heads * SEL, LANES), F32),
            pltpu.VMEM((blocks, heads * SEL, LANES), F32),
            pltpu.VMEM((blocks, heads * SEL, LANES), F32),
            pltpu.VMEM((blocks, heads * SEL, LANES), F32),
            pltpu.VMEM((rows, heads * HEAD), BF16),
            pltpu.VMEM((rows, heads * HEAD), BF16),
            dma((12,)),
            dma((spans,)),
            dma((spans,)),
            dma((spans,)),
            dma((spans,)),
            dma((spans,)),
            dma((spans,)),
            dma((blocks,)),
            dma((blocks,)),
        ],
        compiler_params=pltpu.CompilerParams(collective_id=0, has_side_effects=True),
    )(
        tokens,
        chosen,
        w_query,
        w_ks,
        w_vs,
        w_kc,
        w_vc,
        ski.T,
        sko,
        svi.T,
        svo,
        w_gates.T,
        w_out,
        gain.reshape(1, -1),
    )


def solution(mesh):
    in_specs = (
        P(("dp", "kv"), None),
        P(("dp", "kv"), "tp", None),
        P(None, "tp"),
    ) + (P(),) * 11
    return jax.shard_map(
        functools.partial(local, mesh.shape["kv"]),
        mesh=mesh,
        in_specs=in_specs,
        out_specs=P(("dp", "kv"), "tp"),
        check_vma=False,
    )
```

```python
import functools

import jax
import jax.numpy as jnp
from jax import lax
from jax.experimental import pallas as pl
from jax.experimental.pallas import tpu as pltpu
from jax.sharding import PartitionSpec as P

HEAD = 64
CMP_STRIDE = 16
CMP_LEN = 32
SEL = 64
CAP = 4
FAR = 3
WIDE = 4
LANES = 128
EPS = 1e-06
NEG = -1e30
MESH = pl.DeviceIdType.MESH
F32 = jnp.float32
BF16 = jnp.bfloat16


def dot(a, b):
    return jnp.dot(a, b, preferred_element_type=F32)


def dot_t(a, b):
    return lax.dot_general(a, b, (((1,), (1,)), ((), ())), preferred_element_type=F32)


def swap(x):
    return pltpu.roll(x, HEAD, 1)


def low_lanes(shape):
    return lax.broadcasted_iota(jnp.int32, shape, 1) < HEAD


def kernel(
    spans,
    tokens_h,
    chosen_ref,
    wq_h,
    wks_h,
    wvs_h,
    wkc_h,
    wvc_h,
    ski_h,
    sko_h,
    svi_h,
    svo_h,
    wg_h,
    wo_h,
    gain_ref,
    out_ref,
    tokens,
    wq,
    wsum,
    wcho,
    ski,
    sko,
    svi,
    svo,
    wg,
    wo,
    raw,
    kv_own,
    kv_all,
    packed,
    asks,
    slots,
    pre_all,
    sum_kv,
    q_s,
    gates,
    bias,
    far_bias,
    acc,
    m_s,
    l_s,
    sum_out,
    gate_s,
    mixed_own,
    mixed_other,
    in_sem,
    ask_send,
    ask_recv,
    kv_send,
    kv_recv,
    pre_send,
    pre_recv,
    mix_send,
    mix_recv,
):
    me = lax.axis_index("kv")
    group = lax.axis_index("tp")
    first = group == 0
    rows, _ = tokens.shape
    blocks = rows // SEL
    cmp_rows = rows // CMP_STRIDE
    heads = wq.shape[1] // HEAD
    q_rows = heads * SEL
    chunks, far_keys = far_bias.shape[0], far_bias.shape[2]
    per_chunk = far_keys // (CAP * SEL)

    loads = [
        pltpu.make_async_copy(src, dst, in_sem.at[i])
        for i, (src, dst) in enumerate(
            [
                (wkc_h, wcho.at[:, pl.ds(0, LANES)]),
                (wvc_h, wcho.at[:, pl.ds(LANES, LANES)]),
                (tokens_h, tokens),
                (wks_h, wsum.at[:, pl.ds(0, LANES)]),
                (wvs_h, wsum.at[:, pl.ds(LANES, LANES)]),
                (ski_h, ski),
                (svi_h, svi),
                (wq_h, wq),
                (wg_h, wg),
                (sko_h, sko),
                (svo_h, svo),
                (wo_h, wo),
            ]
        )
    ]
    for load in loads:
        load.start()

    barrier = pltpu.get_barrier_semaphore()

    def greet(step, carry):
        other = lax.rem(me + step, spans)
        pl.semaphore_signal(barrier, inc=1, device_id={"kv": other}, device_id_type=MESH)
        return carry

    lax.fori_loop(1, spans, greet, 0)
    pl.semaphore_signal(barrier, inc=1, device_id={"tp": 1 - group}, device_id_type=MESH)

    low = low_lanes((rows, LANES))

    def ask_copy(source, target):
        return pltpu.make_async_remote_copy(
            src_ref=chosen_ref,
            dst_ref=asks.at[source],
            send_sem=ask_send.at[target],
            recv_sem=ask_recv.at[source],
            device_id={"kv": target},
            device_id_type=MESH,
        )

    def kv_copy(source, target):
        return pltpu.make_async_remote_copy(
            src_ref=packed.at[target],
            dst_ref=kv_all.at[source],
            send_sem=kv_send.at[target],
            recv_sem=kv_recv.at[source],
            device_id={"kv": target},
            device_id_type=MESH,
        )

    def send_ask(span, carry):
        ask_copy(me, span).start()
        return carry

    def enter():
        pl.semaphore_wait(barrier, spans)
        lax.fori_loop(0, me, send_ask, 0)

    pl.when(me >= spans // 2)(enter)

    def block_of_slot(picks):
        lanes = -(-spans * blocks // LANES) * LANES
        ids = lax.broadcasted_iota(jnp.int32, (blocks, lanes), 1)
        hit = jnp.zeros((blocks, lanes), jnp.int32)
        for t in range(picks.shape[1]):
            hit = jnp.where(picks[:, t : t + 1] == ids, 1, hit)
        need = jnp.broadcast_to(jnp.max(hit, axis=0, keepdims=True), (8, lanes))
        lane = lax.broadcasted_iota(jnp.int32, (8, lanes), 1)
        rank = jnp.zeros((8, lanes), jnp.int32)
        for d in range(1, blocks):
            rank = rank + jnp.where(lane % blocks >= d, pltpu.roll(need, d, 1), 0)
        code = jnp.where((need > 0) & (rank < CAP), lane // blocks * CAP + rank, -1)[:1]
        place = lax.broadcasted_iota(jnp.int32, (slots.shape[0], lanes), 0)
        id_row = lax.broadcasted_iota(jnp.int32, (slots.shape[0], lanes), 1)
        found = jnp.where(code == place, id_row, -1)
        return jnp.broadcast_to(jnp.max(found, axis=1, keepdims=True), slots.shape)

    def pair(both):
        k2, v2 = both[:, :LANES], both[:, LANES:]
        k_side = jnp.where(first, k2, swap(k2))
        v_side = jnp.where(first, swap(v2), v2)
        return jnp.where(low, k_side, v_side)

    for load in loads[:3]:
        load.wait()
    kv_own[...] = pair(dot(tokens[...], wcho[...])).astype(BF16)

    for load in loads[3:5]:
        load.wait()
    raw[...] = pair(dot(tokens[...], wsum[...]))

    for load in loads[5:7]:
        load.wait()
    low_c = low_lanes((cmp_rows, LANES))
    key_tiles, value_tiles = [], []
    for a in range(CMP_STRIDE // 2):
        even = raw[pl.ds(2 * a, cmp_rows, stride=CMP_STRIDE), :]
        odd = raw[pl.ds(2 * a + 1, cmp_rows, stride=CMP_STRIDE), :]
        key_tiles.append(jnp.where(low_c, even, swap(odd)).astype(BF16))
        value_tiles.append(jnp.where(low_c, swap(even), odd).astype(BF16))
    half = CMP_STRIDE * HEAD
    joined_k = jnp.concatenate(key_tiles, axis=1)
    joined_v = jnp.concatenate(value_tiles, axis=1)
    head_sum = jnp.concatenate(
        [dot_t(joined_k, ski[:, pl.ds(0, half)]), dot_t(joined_v, svi[:, pl.ds(0, half)])], axis=1
    )
    tail_sum = jnp.concatenate(
        [dot_t(joined_k, ski[:, pl.ds(half, half)]), dot_t(joined_v, svi[:, pl.ds(half, half)])], axis=1
    )
    row_c = lax.broadcasted_iota(jnp.int32, (cmp_rows, LANES), 0)
    shifted = jnp.where(row_c < cmp_rows - 1, pltpu.roll(tail_sum, cmp_rows - 1, 0), 0.0)
    pre_all[me, pl.ds(0, cmp_rows), :] = head_sum + shifted
    pre_all[me, pl.ds(cmp_rows, 8), :] = tail_sum[:8]

    def clear(span, carry):
        pre_all[span] = jnp.zeros(pre_all.shape[1:], F32)
        return carry

    lax.fori_loop(me + 1, spans, clear, 0)

    def pre_copy(source, target):
        return pltpu.make_async_remote_copy(
            src_ref=pre_all.at[source],
            dst_ref=pre_all.at[source],
            send_sem=pre_send.at[target],
            recv_sem=pre_recv.at[source],
            device_id={"kv": target},
            device_id_type=MESH,
        )

    pl.when(me < spans // 2)(enter)

    def send_pre(step, carry):
        pre_copy(me, spans - 1 - step).start()
        return carry

    lax.fori_loop(0, spans - 1 - me, send_pre, 0)


    for load in loads[7:9]:
        load.wait()
    scaled = dot(tokens[...], wq[...]).astype(BF16).astype(F32) * (HEAD**-0.5)
    for a in range(heads // 2):
        tile = scaled[:, a * LANES : (a + 1) * LANES]
        even = jnp.where(low, tile, 0.0).astype(BF16)
        odd = jnp.where(low, swap(tile), 0.0).astype(BF16)
        q_s[:, pl.ds(2 * a * SEL, SEL), :] = even.reshape(blocks, SEL, LANES)
        q_s[:, pl.ds((2 * a + 1) * SEL, SEL), :] = odd.reshape(blocks, SEL, LANES)
    gate_all = jax.nn.sigmoid(dot_t(tokens[...], wg[...]))
    width = 2 * heads
    gates[...] = jnp.where(first, gate_all[:, :width], gate_all[:, width : 2 * width])

    picks = chosen_ref[:, 0, :]

    def bias_of(ids):
        hit = jnp.zeros((blocks, ids.shape[1]), F32)
        for t in range(picks.shape[1]):
            hit = jnp.where(picks[:, t : t + 1] == ids, 1.0, hit)
        return jnp.where(hit > 0.0, 0.0, NEG)

    def lane_sum(p):
        total = p[:, :LANES]
        for c in range(1, p.shape[1] // LANES):
            total = total + p[:, c * LANES : (c + 1) * LANES]
        return total

    def own_attention():
        bias[...] = bias_of(me * blocks + lax.broadcasted_iota(jnp.int32, (blocks, rows), 1) // SEL)
        lane_q = lax.broadcasted_iota(jnp.int32, (q_rows, LANES), 1)
        row_q = lax.broadcasted_iota(jnp.int32, (q_rows, LANES), 0) % SEL
        for jj in range(blocks // 2):
            keys = kv_own[: (jj + 1) * 2 * SEL]
            for odd in range(2):
                j = 2 * jj + odd
                scores = dot_t(q_s[j], keys) + bias[j : j + 1, : keys.shape[0]]
                tail = jnp.where(lane_q <= row_q + odd * SEL, scores[:, -LANES:], NEG)
                if jj > 0:
                    tail = jnp.concatenate([scores[:, :-LANES], tail], axis=1)
                peak = jnp.max(tail, axis=1, keepdims=True)
                p = jnp.exp(tail - peak)
                m_s[j] = jnp.broadcast_to(peak, (q_rows, LANES))
                l_s[j] = lane_sum(p)
                acc[j] = dot(p.astype(BF16), keys)

    pl.when(me == 0)(own_attention)

    def serve(step, carry):
        target = me + 1 + step
        ask_copy(target, me).wait_recv()
        slots[...] = block_of_slot(asks[target][:, 0, :])
        key_lane = lax.broadcasted_iota(jnp.int32, (SEL, rows), 1)
        key_row = lax.broadcasted_iota(jnp.int32, (SEL, rows), 0)
        ours = slots[pl.ds(me * CAP, CAP), :]
        pieces = []
        for k in range(CAP):
            start = (ours[k : k + 1, :1] - me * blocks) * SEL
            pieces.append(jnp.where(key_lane == start + key_row, 1.0, 0.0).astype(BF16))
        packed[target] = dot(jnp.concatenate(pieces, axis=0), kv_own[...]).astype(BF16)
        kv_copy(me, target).start()
        return carry

    lax.fori_loop(0, spans - 1 - me, serve, 0)

    pl.when(me > 0)(own_attention)

    slots[...] = block_of_slot(picks)
    low_b = low_lanes((blocks, LANES))
    for c in range(chunks):
        tiles = []
        for span in range(c * per_chunk, (c + 1) * per_chunk):
            ids = slots[pl.ds(span * CAP, CAP), :]
            ids = jnp.where(span < me, ids, -1)
            for a in range(CAP // 2):
                tiles.append(jnp.where(low_b, ids[2 * a : 2 * a + 1], ids[2 * a + 1 : 2 * a + 2]))
        far_bias[c] = bias_of(jnp.concatenate(tiles, axis=1))

    def clear_far(span, carry):
        kv_all[span] = jnp.zeros(kv_all.shape[1:], BF16)
        return carry

    lax.fori_loop(me, chunks * per_chunk, clear_far, 0)

    def await_pre(span, carry):
        pre_copy(span, me).wait_recv()
        return carry

    lax.fori_loop(0, me, await_pre, 0)
    for load in loads[9:11]:
        load.wait()
    parts = []
    for span in range(spans):
        part = pre_all[span, pl.ds(0, cmp_rows), :]
        if span + 1 < spans:
            part = part + jnp.where(
                row_c == cmp_rows - 1, pre_all[span + 1, pl.ds(cmp_rows, 1), :], 0.0
            )
        parts.append(part)
    hidden = jax.nn.gelu(jnp.concatenate(parts, axis=0)).astype(BF16)
    sum_kv[...] = jnp.concatenate(
        [dot(hidden[:, :HEAD], sko[...]), dot(hidden[:, HEAD:], svo[...])], axis=1
    ).astype(BF16)

    def summarized(j):
        table = sum_kv[...]
        scores = dot_t(q_s[j], table)
        ends = lax.broadcasted_iota(jnp.int32, scores.shape, 1) * CMP_STRIDE + CMP_LEN - 1
        time = me * rows + j * SEL + lax.broadcasted_iota(jnp.int32, scores.shape, 0) % SEL
        visible = ends <= time
        scores = jnp.where(visible, scores, NEG)
        peak = jnp.max(scores, axis=1, keepdims=True)
        p = jnp.where(visible, jnp.exp(scores - peak), 0.0)
        weight = jnp.sum(p, axis=1, keepdims=True)
        gate = gates[j * SEL : (j + 1) * SEL, :]
        near = jnp.concatenate([gate[:, 2 * h : 2 * h + 1] for h in range(heads)], axis=0)
        far = jnp.concatenate([gate[:, 2 * h + 1 : 2 * h + 2] for h in range(heads)], axis=0)
        factor = near / jnp.where(weight > 0.0, weight, 1.0)
        return dot(p.astype(BF16), table) * factor, jnp.broadcast_to(far, (q_rows, LANES))

    for start in range(0, blocks, WIDE):
        some = range(start, start + WIDE)
        for j, (total, far) in zip(some, [summarized(j) for j in some]):
            sum_out[j] = total
            gate_s[j] = far

    def merged(j, chunk):
        keys = kv_all[pl.ds(chunk * per_chunk, per_chunk)].reshape(far_keys, LANES)
        scores = dot_t(q_s[j], keys) + far_bias[chunk, pl.ds(j, 1), :]
        old = m_s[j]
        peak = jnp.maximum(old, jnp.max(scores, axis=1, keepdims=True))
        p = jnp.concatenate(
            [jnp.exp(scores[:, c : c + LANES] - peak) for c in range(0, far_keys, LANES)], axis=1
        )
        fix = jnp.exp(old - peak)
        return peak, l_s[j] * fix + lane_sum(p), acc[j] * fix + dot(p.astype(BF16), keys)

    def await_far(span, carry):
        kv_copy(span, me).wait_recv()
        return carry

    def chunk_step(step, carry):
        chunk = chunks - 1 - step
        lax.fori_loop(
            chunk * per_chunk, jnp.minimum((chunk + 1) * per_chunk, me), await_far, 0
        )

        def update(j, inner):
            peak, weight, total = merged(j, chunk)
            m_s[j] = peak
            l_s[j] = weight
            acc[j] = total
            return inner

        return lax.fori_loop(0, blocks, update, carry)

    if chunks > 1:
        lax.fori_loop(0, chunks - 1, chunk_step, 0)

    lax.fori_loop(0, jnp.minimum(per_chunk, me), await_far, 0)
    low_q = low_lanes((SEL, LANES))

    def mix_copy(j):
        part = pl.ds(pl.multiple_of(j * SEL, SEL), SEL)
        return pltpu.make_async_remote_copy(
            src_ref=mixed_own.at[part, :],
            dst_ref=mixed_other.at[part, :],
            send_sem=mix_send.at[j],
            recv_sem=mix_recv.at[j],
            device_id={"tp": 1 - group},
            device_id_type=MESH,
        )

    def finished(j, far):
        _, weight, total = merged(j, 0) if far else (None, l_s[j], acc[j])
        mixed = sum_out[j] + total * (gate_s[j] / jnp.sum(weight, axis=1, keepdims=True))
        tiles = []
        for a in range(heads // 2):
            even = mixed[2 * a * SEL : (2 * a + 1) * SEL]
            odd = mixed[(2 * a + 1) * SEL : (2 * a + 2) * SEL]
            tiles.append(jnp.where(low_q, swap(even), odd))
        return jnp.concatenate(tiles, axis=1).astype(BF16)

    def finish_all(far):
        for start in range(0, blocks, WIDE):
            some = range(start, start + WIDE)
            for j, mixed in zip(some, [finished(j, far) for j in some]):
                mixed_own[j * SEL : (j + 1) * SEL, :] = mixed
            for j in some:
                mix_copy(j).start()

    pl.when(me == 0)(functools.partial(finish_all, False))
    pl.when(me > 0)(functools.partial(finish_all, True))
    loads[11].wait()

    half_rows = heads * HEAD
    half_cols = wo.shape[1] // 2
    own_rows = pl.ds(pl.multiple_of(group * half_rows, half_rows), half_rows)
    other_rows = pl.ds(pl.multiple_of((1 - group) * half_rows, half_rows), half_rows)
    own_cols = pl.ds(pl.multiple_of(group * half_cols, half_cols), half_cols)
    other_cols = pl.ds(pl.multiple_of((1 - group) * half_cols, half_cols), half_cols)

    gain = gain_ref[:, own_cols]
    for start in range(0, blocks, WIDE):
        for j in range(start, start + WIDE):
            mix_copy(j).wait_recv()
        part = pl.ds(start * SEL, WIDE * SEL)
        own, other = mixed_own[part, :], mixed_other[part, :]
        mine = dot(own, wo[own_rows, own_cols]) + dot(other, wo[other_rows, own_cols])
        rest = dot(own, wo[own_rows, other_cols]) + dot(other, wo[other_rows, other_cols])
        power = jnp.sum(mine * mine + rest * rest, axis=1, keepdims=True)
        out_ref[part, :] = (mine * lax.rsqrt(power / wo.shape[1] + EPS) * gain).astype(BF16)

    def end_mix(j, carry):
        mix_copy(j).wait_send()
        return carry

    lax.fori_loop(0, blocks, end_mix, 0)

    def end_sends(step, carry):
        pre_copy(me, spans - 1 - step).wait_send()
        kv_copy(me, spans - 1 - step).wait_send()
        return carry

    lax.fori_loop(0, spans - 1 - me, end_sends, 0)

    def end_asks(span, carry):
        ask_copy(me, span).wait_send()
        return carry

    lax.fori_loop(0, me, end_asks, 0)


def local(spans, tokens, chosen, *weights):
    w_query, w_ks, w_vs, w_kc, w_vc, ski, sko, svi, svo, w_gates, w_out, gain = weights
    rows, width = tokens.shape
    heads = w_query.shape[1] // HEAD
    blocks = rows // SEL
    cmp_rows = rows // CMP_STRIDE
    per_chunk = min(FAR, spans - 1)
    chunks = -(-(spans - 1) // per_chunk)
    any_spec = pl.BlockSpec(memory_space=pl.ANY)
    vmem = pl.BlockSpec(memory_space=pltpu.VMEM)
    dma = pltpu.SemaphoreType.DMA
    return pl.pallas_call(
        functools.partial(kernel, spans),
        out_shape=jax.ShapeDtypeStruct((rows, w_out.shape[1] // 2), BF16),
        in_specs=[any_spec, vmem] + [any_spec] * 11 + [vmem],
        out_specs=vmem,
        scratch_shapes=[
            pltpu.VMEM(tokens.shape, BF16),
            pltpu.VMEM(w_query.shape, BF16),
            pltpu.VMEM((width, 2 * w_ks.shape[1]), BF16),
            pltpu.VMEM((width, 2 * w_kc.shape[1]), BF16),
            pltpu.VMEM(ski.shape[::-1], BF16),
            pltpu.VMEM(sko.shape, BF16),
            pltpu.VMEM(svi.shape[::-1], BF16),
            pltpu.VMEM(svo.shape, BF16),
            pltpu.VMEM(w_gates.shape[::-1], BF16),
            pltpu.VMEM(w_out.shape, BF16),
            pltpu.VMEM((rows, LANES), F32),
            pltpu.VMEM((rows, LANES), BF16),
            pltpu.VMEM((chunks * per_chunk, CAP * SEL, LANES), BF16),
            pltpu.VMEM((spans, CAP * SEL, LANES), BF16),
            pltpu.VMEM((spans,) + chosen.shape, jnp.int32),
            pltpu.VMEM((max(spans, chunks * per_chunk) * CAP, LANES), jnp.int32),
            pltpu.VMEM((spans, cmp_rows + 8, LANES), F32),
            pltpu.VMEM((spans * cmp_rows, LANES), BF16),
            pltpu.VMEM((blocks, heads * SEL, LANES), BF16),
            pltpu.VMEM((rows, 2 * heads), F32),
            pltpu.VMEM((blocks, rows), F32),
            pltpu.VMEM((chunks, blocks, per_chunk * CAP * SEL), F32),
            pltpu.VMEM((blocks, heads * SEL, LANES), F32),
            pltpu.VMEM((blocks, heads * SEL, LANES), F32),
            pltpu.VMEM((blocks, heads * SEL, LANES), F32),
            pltpu.VMEM((blocks, heads * SEL, LANES), F32),
            pltpu.VMEM((blocks, heads * SEL, LANES), F32),
            pltpu.VMEM((rows, heads * HEAD), BF16),
            pltpu.VMEM((rows, heads * HEAD), BF16),
            dma((12,)),
            dma((spans,)),
            dma((spans,)),
            dma((spans,)),
            dma((spans,)),
            dma((spans,)),
            dma((spans,)),
            dma((blocks,)),
            dma((blocks,)),
        ],
        compiler_params=pltpu.CompilerParams(collective_id=0, has_side_effects=True),
    )(
        tokens,
        chosen,
        w_query,
        w_ks,
        w_vs,
        w_kc,
        w_vc,
        ski.T,
        sko,
        svi.T,
        svo,
        w_gates.T,
        w_out,
        gain.reshape(1, -1),
    )


def solution(mesh):
    in_specs = (
        P(("dp", "kv"), None),
        P(("dp", "kv"), "tp", None),
        P(None, "tp"),
    ) + (P(),) * 11
    return jax.shard_map(
        functools.partial(local, mesh.shape["kv"]),
        mesh=mesh,
        in_specs=in_specs,
        out_specs=P(("dp", "kv"), "tp"),
        check_vma=False,
    )
```
